32 devices in a mesh: fs: 16 (over z, y, x), tp: 2 (over core).
Axes of the slice: x: 2, y: 2, z: 4, core: 2. Of those that a mesh axis runs over, the one named last changes fastest.
Arguments:
- inputs: bfloat16 [8192, 2048], P('fs', 'tp'), may hold values from -6 to 6
- hidden_pre: bfloat16 [8192, 4096], P('fs', 'tp'), may hold values from -6 to 6
- norm_input: bfloat16 [8192, 2048], P('fs', 'tp'), may hold values from -48 to 48, as said below
- out_gain: float32 [2048], P('tp'), may hold values from 0.1 to 1.9
- w_up: bfloat16 [2048, 4096], P('tp', 'fs'), may hold values from -0.125 to 0.125
- w_down: bfloat16 [4096, 2048], P('tp', 'fs'), may hold values from -0.09375 to 0.09375
- cotangent: bfloat16 [8192, 2048], P('fs', 'tp'), may hold values from -6 to 6
Outputs:
- grad_input: bfloat16 [8192, 2048], P('fs', 'tp')
- grad_up: float32 [2048, 4096], P('tp', 'fs')
- grad_gain: float32 [2048], P('tp')
The draws below stay inside these ranges and needn't reach their ends.
Inputs may be any that keep to these rules, and one draw needn't show every extreme that they name: `norm_input`: each token's features are scaled by a factor of that token, and each block of 2048 / 2 features by a factor of that block.
All inputs are finite; a program needn't handle non-finite values.
Results may differ from the reference program's by a relative error of at most 0.0058.
Values may be sent and summed in bfloat16 or wider, within the bound.
A program may use at most 64 MiB of HBM per device.

```python
import jax
import jax.numpy as jnp
from jax import lax

D = 2048
FF = 4096
TOKENS = 8192
N_TP = 2


def draw_norm_input(key, part):
    key_base, key_block, key_row, key_common = jax.random.split(key, 4)
    base = jnp.clip(jax.random.normal(key_base, (TOKENS, D), jnp.float32), -6.0, 6.0)
    blocks = jnp.exp(jax.random.uniform(key_block, (N_TP,), jnp.float32, -1.2, 1.2))
    columns = jnp.repeat(blocks, D // N_TP)
    rowwise = jnp.exp(jax.random.uniform(key_row, (TOKENS, 1), jnp.float32, -0.7, 0.7))
    return (base * rowwise * columns[None, :]).astype(jnp.bfloat16)


def raised(entries, key, source, target, shards_of, factor):
    def block_of(dim):
        return (jnp.arange(entries.shape[dim]) // (entries.shape[dim] // shards_of)).reshape((-1,) + (1,) * (entries.ndim - 1 - dim))

    one_side = jax.random.permutation(key, shards_of)[block_of(target)]
    other_side = (block_of(target) + shards_of // 2) % shards_of
    return jnp.where((block_of(source) == one_side) | (block_of(source) == other_side), factor * entries, entries)


def block_scale(rng, dims, pieces, least, largest):
    factor_of = 1.0
    for position, blocks in pieces:
        draws = jax.random.uniform(jax.random.fold_in(jax.random.fold_in(rng, 6), position), (blocks,), jnp.float32, least / len(pieces), largest / len(pieces))
        factor_of = factor_of * jnp.repeat(jnp.exp(draws), dims[position] // blocks).reshape((-1,) + (1,) * (len(dims) - 1 - position))
    return factor_of


def normal_values(key, dims, deviation, limit, pieces=(), dtype=jnp.bfloat16):
    level = block_scale(key, dims, pieces, -0.22, 0.18) if pieces else 1.0
    entries = jax.random.normal(key, dims, jnp.float32) * deviation * level
    return jnp.minimum(jnp.maximum(entries, -limit), limit).astype(dtype)


def noise_with(own_key, dims, width, bound, cuts, heavy, held_as=jnp.bfloat16):
    result = width * jax.random.normal(own_key, dims, jnp.float32)
    if cuts:
        result = result * block_scale(own_key, dims, cuts, -0.22, 0.18)
    return jnp.clip(raised(result, jax.random.fold_in(own_key, 3), *heavy), -bound, bound).astype(held_as)


def setup_inputs(seed: int = 0) -> dict:
    arg_keys = jax.random.split(jax.random.key(seed), 8)
    inputs = normal_values(arg_keys[0], (TOKENS, D), 1.0, 6.0, ((0, 16), (1, 2)))
    hidden_pre = normal_values(arg_keys[1], (TOKENS, FF), 1.0, 6.0, ((0, 16), (1, 2)))
    norm_input = draw_norm_input(jax.random.fold_in(arg_keys[7], 71), 0)
    out_gain = jnp.clip(1.0 + 0.18 * jax.random.normal(arg_keys[3], (D,), jnp.float32), 0.1, 1.9)
    w_up = normal_values(arg_keys[4], (D, FF), D ** -0.5, 0.125, ((0, 2), (1, 16)))
    w_down = normal_values(arg_keys[5], (FF, D), FF ** -0.5, 0.09375, ((0, 2), (1, 16)))
    cotangent = noise_with(arg_keys[6], (TOKENS, D), 1.0, 6.0, ((0, 16), (1, 2)), (0, 1, 16, 2.0))
    return dict(inputs=inputs, hidden_pre=hidden_pre, norm_input=norm_input, out_gain=out_gain, w_up=w_up, w_down=w_down, cotangent=cotangent)


norm_eps = 1e-06

def reference(inputs, hidden_pre, norm_input, out_gain, w_up, w_down, cotangent):
    scaled = TOKENS ** (-0.5)
    normed = norm_input.astype(jnp.float32)
    upstream = cotangent.astype(jnp.float32)
    inv_rms = lax.rsqrt(lax.optimization_barrier(jnp.mean(normed * normed, axis=1, keepdims=True)) + norm_eps)
    cross_mean = lax.optimization_barrier(jnp.mean(upstream * out_gain * normed, axis=1, keepdims=True))
    d_out = (upstream * out_gain * inv_rms - normed * inv_rms * inv_rms * inv_rms * cross_mean).astype(jnp.bfloat16)
    grad_gain = lax.optimization_barrier(jnp.sum(upstream * normed * inv_rms, axis=0)) * scaled
    d_act = jnp.dot(d_out, w_down.T, preferred_element_type=jnp.float32)
    d_pre = (d_act * 2.0 * jax.nn.relu(hidden_pre.astype(jnp.float32))).astype(jnp.bfloat16)
    grad_input = jnp.dot(d_pre, w_up.T, preferred_element_type=jnp.float32).astype(jnp.bfloat16)
    grad_up = jnp.dot(inputs.T, d_pre, preferred_element_type=jnp.float32) * scaled
    return (grad_input, grad_up, grad_gain)
```

```python
import functools

import jax
import jax.numpy as jnp
from jax import lax
from jax.experimental import pallas as pl
from jax.experimental.pallas import tpu as pltpu
from jax.sharding import PartitionSpec as P


norm_eps = 1e-06
MESH = pl.DeviceIdType.MESH
SEMS = 256


def trade(x, axis, mask):
    if mask == 0:
        return x
    return lax.ppermute(x, axis, [(i, i ^ mask) for i in range(lax.axis_size(axis))])


def total(x, axis):
    step = 1
    while step < lax.axis_size(axis):
        x = x + trade(x, axis, step)
        step *= 2
    return x


def masks_of(n):
    masks = [1 << i for i in range(n.bit_length() - 1)]
    return (masks, masks[::-1])


def halves(x):
    rows = x.shape[0] // 2
    return (x[:rows], x[rows:])


def gather_near(x, near_n):
    parts = []
    for part, masks in zip(halves(x), masks_of(near_n)):
        held = {0: part}
        for mask in masks:
            held.update({k ^ mask: trade(v, "fs", mask) for k, v in list(held.items())})
        parts.append(held)
    return parts


def scatter_near(pieces, near_n):
    sums = []
    for side, masks in enumerate(masks_of(near_n)):
        held = {k: halves(v)[side] for k, v in pieces.items()}
        for mask in masks:
            sent = {k: held.pop(k) for k in list(held) if k & mask}
            for k, v in sent.items():
                came = trade(v.astype(jnp.bfloat16), "fs", mask).astype(jnp.float32)
                held[k ^ mask] = held[k ^ mask] + came
        sums.append(held[0])
    return jnp.concatenate(sums, axis=0)


def tree(x, n, unit):
    terms = [trade(x, "fs", k * unit) for k in range(n)]
    while len(terms) > 1:
        terms = [a + b for a, b in zip(terms[::2], terms[1::2])]
    return terms[0]


def pick(stack, index):
    return lax.dynamic_index_in_dim(stack, index, 0, keepdims=False)


def dot(a, b, dim):
    return lax.dot_general(
        a, b, (((dim,), (dim,)), ((), ())), preferred_element_type=jnp.float32
    )


def on_device(inputs, hidden_pre, norm_input, out_gain, w_up, w_down, cotangent):
    fs, tp = lax.axis_size("fs"), lax.axis_size("tp")
    near_n = 1
    while 4 * near_n * near_n <= fs:
        near_n *= 2
    far_n = fs // near_n
    per = far_n // tp
    me, core = lax.axis_index("fs"), lax.axis_index("tp")
    far, near = me // near_n, me % near_n
    rows = inputs.shape[0]
    width = inputs.shape[1] * tp
    scaled = (rows * fs) ** (-0.5)
    block = w_up.shape[1]
    cols = w_down.shape[1]

    down_rows = w_down.reshape(per, near_n, block, cols)
    asked = [
        lax.dynamic_index_in_dim(down_rows, near ^ k, 1, keepdims=False).reshape(per * block, cols)
        for k in range(near_n)
    ]
    arrived = [trade(x, "fs", k) for k, x in enumerate(asked)]
    arrived = jnp.stack(arrived)
    down_near = jnp.concatenate([pick(arrived, near ^ i) for i in range(near_n)], axis=1)
    down_far = [trade(down_near, "fs", k * near_n) for k in range(far_n)]
    up_far = [trade(w_up, "fs", k * near_n) for k in range(far_n)]
    up_far = jnp.stack(up_far)
    down_far = jnp.stack(down_far)
    down, up = [], []
    for t in range(tp):
        places = [((core ^ t) * per + j) ^ far for j in range(per)]
        down.append(jnp.concatenate([pick(down_far, i) for i in places], axis=1))
        up.append(jnp.concatenate([pick(up_far, i) for i in places], axis=1))

    asked = [
        jnp.concatenate(
            [
                lax.dynamic_slice_in_dim(
                    hidden_pre, (j * near_n + (near ^ k)) * block, block, axis=1
                )
                for j in range(per)
            ],
            axis=1,
        )
        for k in range(near_n)
    ]
    pre = [trade(x, "fs", k) for k, x in enumerate(asked)]

    normed = norm_input.astype(jnp.float32)
    upstream = cotangent.astype(jnp.float32)
    weighted = upstream * out_gain
    sums = total(
        jnp.stack([jnp.sum(normed * normed, axis=1), jnp.sum(weighted * normed, axis=1)]), "tp"
    )
    inv_rms = lax.rsqrt(sums[0] / width + norm_eps)[:, None]
    cross_mean = (sums[1] / width)[:, None]
    d_out = (weighted * inv_rms - normed * inv_rms * inv_rms * inv_rms * cross_mean).astype(
        jnp.bfloat16
    )
    gain = jnp.sum(upstream * normed * inv_rms, axis=0) * scaled
    gain = tree(gain, near_n, 1)
    grad_gain = tree(gain, far_n, near_n)

    d_outs = gather_near(d_out, near_n)
    tokens = gather_near(inputs, near_n)
    d_pres, partial = [], {}
    for k in range(near_n):
        d_out_k = jnp.concatenate([d_outs[0][k], d_outs[1][k]], axis=0)
        d_out_k = [trade(d_out_k, "tp", t) for t in range(tp)]
        d_act = sum(dot(d_out_k[t], down[t], 1) for t in range(tp))
        d_pre = (d_act * 2.0 * jax.nn.relu(pre[k].astype(jnp.float32))).astype(jnp.bfloat16)
        d_pres.append([trade(d_pre, "tp", t) for t in range(tp)])
        partial[k] = sum(dot(d_pres[k][t], up[t], 1) for t in range(tp))
    grad_input = scatter_near(partial, near_n)

    all_pres = [
        jnp.concatenate([d_pres[k][t] for k in range(near_n)], axis=0) for t in range(tp)
    ]
    all_tokens = jnp.concatenate([side[k] for k in range(near_n) for side in tokens], axis=0)
    sums_up = [dot(x, all_tokens, 0) for x in all_pres]
    sums_up = jnp.concatenate(sums_up, axis=0).reshape(
        far_n, block, inputs.shape[1]
    )
    grad_up = 0.0
    for k in range(far_n):
        goal = far ^ k
        mine = pick(sums_up, (core ^ (goal // per)) * per + goal % per)
        if k:
            mine = trade(mine.astype(jnp.bfloat16), "fs", k * near_n).astype(jnp.float32)
        grad_up = grad_up + mine
    return (grad_input.astype(jnp.bfloat16), (grad_up * scaled).T, grad_gain)


def mm(a, b):
    return lax.dot_general(a, b, (((1,), (1,)), ((), ())), preferred_element_type=jnp.float32)


class Wire:
    def __init__(self, send, recv, other):
        self.send, self.recv, self.other = send, recv, other
        self.sent, self.came, self.pending = {}, {}, []

    def at(self, sems, names, key):
        index = names.setdefault(key, len(names))
        assert index < sems.shape[0], "semaphores"
        return sems.at[index]

    def put(self, refs, key, device, live=None, tag=None):
        out = self.at(self.send, self.sent, (key, tag))
        arrival = self.at(self.recv, self.came, key)

        def copy():
            source, target = refs()
            return pltpu.make_async_remote_copy(
                src_ref=source, dst_ref=target, send_sem=out, recv_sem=arrival,
                device_id=device, device_id_type=MESH,
            )

        when(live, lambda: copy().start())
        self.pending.append((copy, live))

    def got(self, ref, key):
        pltpu.make_async_remote_copy(
            src_ref=ref, dst_ref=ref, send_sem=self.send.at[0],
            recv_sem=self.at(self.recv, self.came, key),
            device_id=self.other, device_id_type=MESH,
        ).wait_recv()

    def drain(self):
        for copy, live in self.pending:
            when(live, lambda: copy().wait_send())
        self.pending = []


def when(live, body):
    if live is None:
        body()
    else:
        pl.when(live)(body)


def both(a, b):
    return a if b is None else b if a is None else jnp.logical_and(a, b)


def fused(nz, ny, inp, pre, nrm, gain, wu, wd, cot, gi_out, gu_out, gg_out,
          nrm_v, cot_v, gain_v, st, st2, d_out, inp_v, inp_t, pre_v, dn, up, dp,
          part, gi_own, gi_send, gi_got, chain, y_send, y_got, acc, gu_v,
          gacc, gx, gx2, gy, gy2, gz, loc, send, recv):
    nx, f32, bf16 = 2, jnp.float32, jnp.bfloat16
    rows, half = inp.shape
    nq, _, blk, cols = wd.shape
    ns = nz * ny
    width = 2 * half
    wide = nx * cols
    chunks = 4
    step = rows // chunks
    high = half // nq
    scaled = (rows * nz * ny * nx) ** (-0.5)

    me, core = lax.axis_index("fs"), lax.axis_index("tp")
    x, y, z = me % nx, (me // nx) % ny, me // (nx * ny)
    at_x = (me + 1 - 2 * x, core)
    at_y = (me + nx * (1 - 2 * y), core)
    at_up = (me + nx * ny, core)
    at_down = (me - nx * ny, core)
    at_core = (me, 1 - core)
    at_z = [(lax.rem(z + k, nz) * nx * ny + y * nx + x, core) for k in range(1, nz)]
    wire = Wire(send, recv, at_core)
    low_end, top_end = z > 0, z < nz - 1

    def place(zz, yy):
        return lax.rem(zz * ny + yy + core * nq, ns)

    local = {}

    def load(name, refs):
        index = len(local)
        local[name] = (lambda: pltpu.make_async_copy(*refs(), loc.at[index]))
        local[name]().start()

    def ready(name):
        local[name]().wait()

    load("nrm", lambda: (nrm, nrm_v))
    load("cot", lambda: (cot, cot_v))
    load("gain", lambda: (gain, gain_v))

    def own_dn(q, xx):
        start = place(z, y) * wide + xx * cols
        return dn.at[pl.ds(q * blk, blk), pl.ds(pl.multiple_of(start, cols), cols)]

    for q in range(nq):
        load(("dn", q), lambda q=q: (wd.at[q, x], own_dn(q, x)))
    for q in range(nq):
        load(("up", q), lambda q=q: (
            wu.at[pl.ds(q * high, high), :],
            up.at[pl.ds(q * high, high), pl.ds(pl.multiple_of(place(z, y) * blk, blk), blk)]))
    for q in range(nq):
        load(("pre", q), lambda q=q: (
            pre.at[:, pl.ds(pl.multiple_of((2 * q + x) * blk, blk), blk)], pre_v.at[0, q]))
    load("inp", lambda: (inp, inp_v.at[0]))

    barrier = pltpu.get_barrier_semaphore()
    peers = [at_core, at_x, at_y] + at_z
    for peer in peers:
        pl.semaphore_signal(barrier, inc=1, device_id=peer, device_id_type=MESH)
    pl.semaphore_wait(barrier, len(peers))

    for q in range(nq):
        wire.put(lambda q=q: (wd.at[q, 1 - x], own_dn(q, x)), ("swap", q), at_x)

    ready("nrm")
    ready("cot")
    ready("gain")
    gacc[...] = jnp.zeros_like(gacc)
    tall = 32

    def stats(i, carry):
        r = pl.ds(pl.multiple_of(i * tall, tall), tall)
        n = nrm_v[r, :].astype(f32)
        u = cot_v[r, :].astype(f32) * gain_v[...]
        squares = jnp.sum(n * n, axis=1, keepdims=True)
        cross = jnp.sum(u * n, axis=1, keepdims=True)
        lane = lax.broadcasted_iota(jnp.int32, (tall, st.shape[1]), 1)
        st[r, :] = jnp.where(lane == 0, squares, cross)
        return carry

    lax.fori_loop(0, rows // tall, stats, 0)
    wire.put(lambda: (st, st2), "stats", at_core)

    def piece(buf, tile, w, j, zz, yy):
        return buf.at[pl.ds(j * tile, tile), pl.ds(pl.multiple_of(place(zz, yy) * w, w), w)]

    gathers = {"dn": (dn, blk, wide), "up": (up, high, blk)}

    def spread(name, j, zz, tag, live, up_key, down_key, to_y=True, to_z=True):
        refs = lambda: (piece(*gathers[name], j, zz, y),) * 2
        if to_z and up_key is not None:
            wire.put(refs, (name, j, "u", up_key), at_up, both(live, top_end), tag)
        if to_z and down_key is not None:
            wire.put(refs, (name, j, "d", down_key), at_down, both(live, low_end), tag)
        if to_y:
            wire.put(refs, (name, j, "y", tag), at_y, live, "y")

    def own(name, j, **kw):
        spread(name, j, z, "own", None, 1, 1, **kw)

    def forward(name, j, k):
        below, above = z >= k, z + k < nz
        when(below, lambda: wire.got(piece(*gathers[name], j, z - k, y), (name, j, "u", k)))
        spread(name, j, z - k, ("u", k), below, k + 1 if k + 1 < nz else None, None)
        when(above, lambda: wire.got(piece(*gathers[name], j, z + k, y), (name, j, "d", k)))
        spread(name, j, z + k, ("d", k), above, None, k + 1 if k + 1 < nz else None)

    def arrived(name, j):
        wire.got(piece(*gathers[name], j, z, 1 - y), (name, j, "y", "own"))
        for k in range(1, nz):
            when(z >= k, lambda: wire.got(
                piece(*gathers[name], j, z - k, 1 - y), (name, j, "y", ("u", k))))
            when(z + k < nz, lambda: wire.got(
                piece(*gathers[name], j, z + k, 1 - y), (name, j, "y", ("d", k))))

    ready(("dn", 0))
    wire.got(own_dn(0, 1 - x), ("swap", 0))
    own("dn", 0)

    wire.got(st2, "stats")
    short = 16

    def norm(n_chunk):
        def rows_of(i, carry):
            r = pl.ds(pl.multiple_of(n_chunk * step + i * short, short), short)
            n = nrm_v[r, :].astype(f32)
            u = cot_v[r, :].astype(f32)
            both_sums = st[r, :] + st2[r, :]
            inv = lax.rsqrt(both_sums[:, 0:1] / width + norm_eps)
            cross = both_sums[:, 1:2] / width
            d = u * gain_v[...] * inv - n * (inv * inv * inv * cross)
            d_out[r, pl.ds(0, half)] = d.astype(bf16)
            g = u * n * inv
            gacc[...] += g[0:8] + g[8:16]
            return carry

        lax.fori_loop(0, step // short, rows_of, 0)

    def d_tile(t, n_chunk, h):
        return d_out.at[pl.ds(t * rows + n_chunk * step, step), pl.ds(h * half, half)]

    for n in range(chunks):
        norm(n)
        wire.put(lambda n=n: (d_tile(0, n, 0), d_tile(1, n, 0)), ("d_x", n), at_x)
        wire.put(lambda n=n: (d_tile(0, n, 0), d_tile(0, n, 1)), ("d_core", 0, n), at_core)

    for q in range(1, nq):
        ready(("dn", q))
        wire.got(own_dn(q, 1 - x), ("swap", q))
        own("dn", q)

    for q in range(nq):
        wire.put(lambda q=q: (
            pre.at[:, pl.ds(pl.multiple_of((2 * q + 1 - x) * blk, blk), blk)], pre_v.at[1, q]),
            ("pre", q), at_x)
    gx[...] = jnp.sum(gacc[...], axis=0, keepdims=True)
    wire.put(lambda: (gx, gx2), "gain_x", at_x)
    wire.put(lambda: (inp, inp_v.at[1]), "inp", at_x)

    def turn(t):
        def cols_of(i, carry):
            c = pl.ds(pl.multiple_of(i * blk, blk), blk)
            for k in range(half // blk):
                inp_t[pl.ds(k * blk, blk), pl.ds(pl.multiple_of(t * rows + i * blk, blk), blk)] = (
                    inp_v[t, c, pl.ds(k * blk, blk)].T)
            return carry

        lax.fori_loop(0, rows // blk, cols_of, 0)

    def act(t, q):
        def rows_of(i, carry):
            r = pl.ds(pl.multiple_of(t * rows + i * blk, blk), blk)
            got = mm(d_out[r, :], dn[pl.ds(q * blk, blk), :])
            p = pre_v[t, q, pl.ds(pl.multiple_of(i * blk, blk), blk), :].astype(f32)
            dp[r, pl.ds(q * blk, blk)] = (got * 2.0 * jnp.maximum(p, 0.0)).astype(bf16)
            return carry

        lax.fori_loop(0, rows // blk, rows_of, 0)
        tile = lambda s: dp.at[pl.ds(t * rows, rows), pl.ds((s * nq + q) * blk, blk)]
        wire.put(lambda: (tile(0), tile(1)), ("dp", t, q), at_core)

    for q in range(nq):
        for k in range(1, nz):
            forward("dn", q, k)
        if q < chunks:
            wire.got(d_tile(1, q, 0), ("d_x", q))
            wire.put(lambda q=q: (d_tile(1, q, 0), d_tile(1, q, 1)), ("d_core", 1, q), at_core)
        if q == 0:
            for n in range(chunks):
                wire.got(d_tile(0, n, 1), ("d_core", 0, n))
            ready("inp")
            turn(0)
        else:
            ready(("pre", q - 1))
            arrived("dn", q - 1)
            act(0, q - 1)
    for q in range(nq):
        ready(("up", q))
        own("up", q)
    ready(("pre", nq - 1))
    arrived("dn", nq - 1)
    act(0, nq - 1)

    wire.got(gx2, "gain_x")
    gy[...] = gx[...] + gx2[...]
    wire.put(lambda: (gy, gy2), "gain_y", at_y)

    for n in range(chunks):
        wire.got(d_tile(1, n, 1), ("d_core", 1, n))
    for q in range(nq):
        wire.got(pre_v.at[1, q], ("pre", q))
        act(1, q)
        for k in range(1, nz):
            forward("up", q, k)

    wire.got(gy2, "gain_y")
    gz[z] = gy[...] + gy2[...]
    for k, peer in enumerate(at_z):
        wire.put(lambda: (gz.at[z], gz.at[z]), ("gain_z", k), peer)

    for t in range(nx):
        for q in range(nq):
            wire.got(dp.at[pl.ds(t * rows, rows), pl.ds((nq + q) * blk, blk)], ("dp", t, q))

    def back(r):
        def rows_of(i, carry):
            k = pl.ds(pl.multiple_of(i * blk, blk), blk)
            w = up[pl.ds(r * high, high), :]
            far = mm(dp[pl.ds(pl.multiple_of(rows + i * blk, blk), blk), :], w)
            gi_send[r, k, :] = far.astype(bf16)
            return carry

        def rows_own(i, carry):
            k = pl.ds(pl.multiple_of(i * blk, blk), blk)
            w = up[pl.ds(r * high, high), :]
            gi_own[r, k, :] = mm(dp[k, :], w)
            return carry

        lax.fori_loop(0, rows // blk, rows_of, 0)
        wire.put(lambda: (gi_send.at[r], gi_got.at[r]), ("gi", r), at_x)
        lax.fori_loop(0, rows // blk, rows_own, 0)

    def grads(r):
        for j in range(ns):
            part[r, j] = lax.dot_general(
                inp_t[pl.ds(r * high, high), :], dp[:, pl.ds(j * blk, blk)],
                (((1,), (0,)), ((), ())), preferred_element_type=f32)

    def column(rel):
        return y if rel == 0 else 1 - y

    def link(kind, r, goal, rel):
        first, live, device = (
            (z == 0, z < goal, at_up) if kind == 0 else (z == nz - 1, z > goal, at_down))
        slot = chain.at[kind, r, goal, rel]
        key = ("sum", kind, r, goal, rel)

        def value():
            got = part[r, place(goal, column(rel))]
            return got + y_got[r, goal].astype(f32) if r >= split else got

        @pl.when(jnp.logical_and(live, first))
        def _():
            slot[...] = value().astype(bf16)

        @pl.when(jnp.logical_and(live, jnp.logical_not(first)))
        def _():
            wire.got(slot, key)
            slot[...] = (value() + slot[...].astype(f32)).astype(bf16)

        wire.put(lambda: (slot, slot), key, device, live)

    def links(r):
        for i in range(nz - 1):
            for rel in range(ny if r < split else 1):
                link(0, r, nz - 1 - i, rel)
                link(1, r, i, rel)

    def collect(r, rel):
        acc[...] = part[r, place(z, column(rel))]
        for kind, live in ((0, z > 0), (1, z < nz - 1)):
            @pl.when(live)
            def _():
                slot = chain.at[kind, r, z, rel]
                for goal in range(nz):
                    when(z == goal, lambda: wire.got(slot, ("sum", kind, r, goal, rel)))
                acc[...] += slot[...].astype(f32)

    def to_y(r, goal):
        y_send[r, goal] = part[r, place(goal, 1 - y)].astype(bf16)
        wire.put(lambda: (y_send.at[r, goal], y_got.at[r, goal]), ("y", r, goal), at_y)

    def finish(r):
        gu_v[pl.ds(r * high, high), :] = acc[...] * scaled
        tile = pl.ds(r * high, high)
        load(("gu", r), lambda: (gu_v.at[tile, :], gu_out.at[tile, :]))

    split = nq // 2
    arrived("up", 0)
    back(0)
    arrived("up", 1)
    back(1)
    wire.got(inp_v.at[1], "inp")
    turn(1)
    for r in range(split):
        grads(r)
        links(r)
    for r in range(split, nq):
        grads(r)
        for goal in range(nz):
            to_y(r, goal)
    for r in range(2, nq):
        arrived("up", r)
        back(r)
    for r in range(split):
        collect(r, 1)
        y_send[r, 0] = acc[...].astype(bf16)
        wire.put(lambda r=r: (y_send.at[r, 0], y_got.at[r, 0]), ("y", r, 0), at_y)
    for r in range(split, nq):
        for goal in range(nz):
            wire.got(y_got.at[r, goal], ("y", r, goal))
        links(r)
    for k in range(nz - 1):
        source = lax.rem(z + nz - 1 - k, nz)
        wire.got(gz.at[source], ("gain_z", k))
    total = gz[0]
    for k in range(1, nz):
        total = total + gz[k]
    gx2[...] = total * scaled
    load("gg", lambda: (gx2, gg_out))
    for r in range(nq):
        wire.got(gi_got.at[r], ("gi", r))
        inp_v[0, :, pl.ds(r * high, high)] = (gi_own[r] + gi_got[r].astype(f32)).astype(bf16)
    load("gi", lambda: (inp_v.at[0], gi_out))
    for r in range(split):
        collect(r, 0)
        wire.got(y_got.at[r, 0], ("y", r, 0))
        acc[...] += y_got[r, 0].astype(f32)
        finish(r)
    for r in range(split, nq):
        collect(r, 0)
        acc[...] += y_got[r, z].astype(f32)
        finish(r)
    wire.drain()
    for name in ["gg", "gi"] + [("gu", r) for r in range(nq)]:
        ready(name)


def kernel_step(fs, tp, inputs, hidden_pre, norm_input, out_gain, w_up, w_down, cotangent):
    nx = ny = 2
    nz = fs // (nx * ny)
    rows, half = inputs.shape
    blk, cols = w_up.shape[1], w_down.shape[1]
    nq = nz * ny // tp
    ns, high = nz * ny, half // nq
    hid = nq * blk
    f32, bf16 = jnp.float32, jnp.bfloat16
    v = pltpu.VMEM
    scratch = [
        v((rows, half), bf16), v((rows, half), bf16), v((1, half), f32),
        v((rows, 128), f32), v((rows, 128), f32),
        v((nx * rows, 2 * half), bf16),
        v((nx, rows, half), bf16), v((half, nx * rows), bf16),
        v((nx, nq, rows, blk), bf16),
        v((hid, 2 * half), bf16), v((half, ns * blk), bf16), v((nx * rows, ns * blk), bf16),
        v((nq, ns, high, blk), f32),
        v((nq, rows, high), f32), v((nq, rows, high), bf16), v((nq, rows, high), bf16),
        v((2, nq, nz, ny, high, blk), bf16),
        v((nq, nz, high, blk), bf16), v((nq, nz, high, blk), bf16),
        v((high, blk), f32), v((half, blk), f32),
        v((8, half), f32),
        v((1, half), f32), v((1, half), f32), v((1, half), f32), v((1, half), f32),
        v((nz, 1, half), f32),
        pltpu.SemaphoreType.DMA((3 + 3 * nq + 1 + 2 + nq,)),
        pltpu.SemaphoreType.DMA((SEMS,)), pltpu.SemaphoreType.DMA((SEMS,)),
    ]
    flops = 3 * 2 * nx * rows * 2 * half * hid
    grad_input, grad_up, grad_gain = pl.pallas_call(
        functools.partial(fused, nz, ny),
        out_shape=(
            jax.ShapeDtypeStruct((rows, half), bf16),
            jax.ShapeDtypeStruct((half, blk), f32),
            jax.ShapeDtypeStruct((1, half), f32),
        ),
        in_specs=[pl.BlockSpec(memory_space=pl.ANY)] * 7,
        out_specs=(pl.BlockSpec(memory_space=pl.ANY),) * 3,
        scratch_shapes=scratch,
        compiler_params=pltpu.CompilerParams(
            collective_id=0, has_side_effects=True, vmem_limit_bytes=67_000_000
        ),
        cost_estimate=pl.CostEstimate(flops=flops, bytes_accessed=1 << 24, transcendentals=0),
        name="layer_backward",
    )(
        inputs, hidden_pre, norm_input, out_gain.reshape(1, half), w_up,
        w_down.reshape(nq, nx, blk, cols), cotangent,
    )
    return grad_input, grad_up, grad_gain.reshape(half)


def in_kernel(*args):
    return kernel_step(lax.axis_size("fs"), lax.axis_size("tp"), *args)


def solution(mesh):
    placed = (
        P("fs", "tp"),
        P("fs", "tp"),
        P("fs", "tp"),
        P("tp"),
        P("tp", "fs"),
        P("tp", "fs"),
        P("fs", "tp"),
    )
    fs, tp = mesh.shape["fs"], mesh.shape["tp"]
    out_specs = (P("fs", "tp"), P("tp", "fs"), P("tp"))

    def solve(*args):
        up, down = args[4].shape, args[5].shape
        if tp == 2 and fs % 8 == 0 and up[1] // fs % 256 == 0 and down[1] // fs % 128 == 0:
            return jax.shard_map(
                in_kernel, mesh=mesh, in_specs=placed, out_specs=out_specs, check_vma=False
            )(*args)
        return permuted(*args)

    step = jax.shard_map(
        on_device,
        mesh=mesh,
        in_specs=placed,
        out_specs=(P("fs", "tp"), P("tp", "fs"), P("tp")),
        check_vma=False,
    )
    permuted = step
    return solve
```

```python
import functools

import jax
import jax.numpy as jnp
from jax import lax
from jax.experimental import pallas as pl
from jax.experimental.pallas import tpu as pltpu
from jax.sharding import PartitionSpec as P


norm_eps = 1e-06
MESH = pl.DeviceIdType.MESH
SEMS = 320


def trade(x, axis, mask):
    if mask == 0:
        return x
    return lax.ppermute(x, axis, [(i, i ^ mask) for i in range(lax.axis_size(axis))])


def total(x, axis):
    step = 1
    while step < lax.axis_size(axis):
        x = x + trade(x, axis, step)
        step *= 2
    return x


def masks_of(n):
    masks = [1 << i for i in range(n.bit_length() - 1)]
    return (masks, masks[::-1])


def halves(x):
    rows = x.shape[0] // 2
    return (x[:rows], x[rows:])


def gather_near(x, near_n):
    parts = []
    for part, masks in zip(halves(x), masks_of(near_n)):
        held = {0: part}
        for mask in masks:
            held.update({k ^ mask: trade(v, "fs", mask) for k, v in list(held.items())})
        parts.append(held)
    return parts


def scatter_near(pieces, near_n):
    sums = []
    for side, masks in enumerate(masks_of(near_n)):
        held = {k: halves(v)[side] for k, v in pieces.items()}
        for mask in masks:
            sent = {k: held.pop(k) for k in list(held) if k & mask}
            for k, v in sent.items():
                came = trade(v.astype(jnp.bfloat16), "fs", mask).astype(jnp.float32)
                held[k ^ mask] = held[k ^ mask] + came
        sums.append(held[0])
    return jnp.concatenate(sums, axis=0)


def tree(x, n, unit):
    terms = [trade(x, "fs", k * unit) for k in range(n)]
    while len(terms) > 1:
        terms = [a + b for a, b in zip(terms[::2], terms[1::2])]
    return terms[0]


def pick(stack, index):
    return lax.dynamic_index_in_dim(stack, index, 0, keepdims=False)


def dot(a, b, dim):
    return lax.dot_general(
        a, b, (((dim,), (dim,)), ((), ())), preferred_element_type=jnp.float32
    )


def on_device(inputs, hidden_pre, norm_input, out_gain, w_up, w_down, cotangent):
    fs, tp = lax.axis_size("fs"), lax.axis_size("tp")
    near_n = 1
    while 4 * near_n * near_n <= fs:
        near_n *= 2
    far_n = fs // near_n
    per = far_n // tp
    me, core = lax.axis_index("fs"), lax.axis_index("tp")
    far, near = me // near_n, me % near_n
    rows = inputs.shape[0]
    width = inputs.shape[1] * tp
    scaled = (rows * fs) ** (-0.5)
    block = w_up.shape[1]
    cols = w_down.shape[1]

    down_rows = w_down.reshape(per, near_n, block, cols)
    asked = [
        lax.dynamic_index_in_dim(down_rows, near ^ k, 1, keepdims=False).reshape(per * block, cols)
        for k in range(near_n)
    ]
    arrived = [trade(x, "fs", k) for k, x in enumerate(asked)]
    arrived = jnp.stack(arrived)
    down_near = jnp.concatenate([pick(arrived, near ^ i) for i in range(near_n)], axis=1)
    down_far = [trade(down_near, "fs", k * near_n) for k in range(far_n)]
    up_far = [trade(w_up, "fs", k * near_n) for k in range(far_n)]
    up_far = jnp.stack(up_far)
    down_far = jnp.stack(down_far)
    down, up = [], []
    for t in range(tp):
        places = [((core ^ t) * per + j) ^ far for j in range(per)]
        down.append(jnp.concatenate([pick(down_far, i) for i in places], axis=1))
        up.append(jnp.concatenate([pick(up_far, i) for i in places], axis=1))

    asked = [
        jnp.concatenate(
            [
                lax.dynamic_slice_in_dim(
                    hidden_pre, (j * near_n + (near ^ k)) * block, block, axis=1
                )
                for j in range(per)
            ],
            axis=1,
        )
        for k in range(near_n)
    ]
    pre = [trade(x, "fs", k) for k, x in enumerate(asked)]

    normed = norm_input.astype(jnp.float32)
    upstream = cotangent.astype(jnp.float32)
    weighted = upstream * out_gain
    sums = total(
        jnp.stack([jnp.sum(normed * normed, axis=1), jnp.sum(weighted * normed, axis=1)]), "tp"
    )
    inv_rms = lax.rsqrt(sums[0] / width + norm_eps)[:, None]
    cross_mean = (sums[1] / width)[:, None]
    d_out = (weighted * inv_rms - normed * inv_rms * inv_rms * inv_rms * cross_mean).astype(
        jnp.bfloat16
    )
    gain = jnp.sum(upstream * normed * inv_rms, axis=0) * scaled
    gain = tree(gain, near_n, 1)
    grad_gain = tree(gain, far_n, near_n)

    d_outs = gather_near(d_out, near_n)
    tokens = gather_near(inputs, near_n)
    d_pres, partial = [], {}
    for k in range(near_n):
        d_out_k = jnp.concatenate([d_outs[0][k], d_outs[1][k]], axis=0)
        d_out_k = [trade(d_out_k, "tp", t) for t in range(tp)]
        d_act = sum(dot(d_out_k[t], down[t], 1) for t in range(tp))
        d_pre = (d_act * 2.0 * jax.nn.relu(pre[k].astype(jnp.float32))).astype(jnp.bfloat16)
        d_pres.append([trade(d_pre, "tp", t) for t in range(tp)])
        partial[k] = sum(dot(d_pres[k][t], up[t], 1) for t in range(tp))
    grad_input = scatter_near(partial, near_n)

    all_pres = [
        jnp.concatenate([d_pres[k][t] for k in range(near_n)], axis=0) for t in range(tp)
    ]
    all_tokens = jnp.concatenate([side[k] for k in range(near_n) for side in tokens], axis=0)
    sums_up = [dot(x, all_tokens, 0) for x in all_pres]
    sums_up = jnp.concatenate(sums_up, axis=0).reshape(
        far_n, block, inputs.shape[1]
    )
    grad_up = 0.0
    for k in range(far_n):
        goal = far ^ k
        mine = pick(sums_up, (core ^ (goal // per)) * per + goal % per)
        if k:
            mine = trade(mine.astype(jnp.bfloat16), "fs", k * near_n).astype(jnp.float32)
        grad_up = grad_up + mine
    return (grad_input.astype(jnp.bfloat16), (grad_up * scaled).T, grad_gain)


def mm(a, b):
    return lax.dot_general(a, b, (((1,), (1,)), ((), ())), preferred_element_type=jnp.float32)


class Wire:
    def __init__(self, send, recv, other):
        self.send, self.recv, self.other = send, recv, other
        self.sent, self.came, self.pending = {}, {}, []

    def at(self, sems, names, key):
        index = names.setdefault(key, len(names))
        assert index < sems.shape[0], "semaphores"
        return sems.at[index]

    def put(self, refs, key, device, live=None, tag=None):
        out = self.at(self.send, self.sent, (key, tag))
        arrival = self.at(self.recv, self.came, key)

        def copy():
            source, target = refs()
            return pltpu.make_async_remote_copy(
                src_ref=source, dst_ref=target, send_sem=out, recv_sem=arrival,
                device_id=device, device_id_type=MESH,
            )

        when(live, lambda: copy().start())
        self.pending.append((copy, live))

    def got(self, ref, key):
        pltpu.make_async_remote_copy(
            src_ref=ref, dst_ref=ref, send_sem=self.send.at[0],
            recv_sem=self.at(self.recv, self.came, key),
            device_id=self.other, device_id_type=MESH,
        ).wait_recv()

    def drain(self):
        for copy, live in self.pending:
            when(live, lambda: copy().wait_send())
        self.pending = []


def when(live, body):
    if live is None:
        body()
    else:
        pl.when(live)(body)


def both(a, b):
    return a if b is None else b if a is None else jnp.logical_and(a, b)


def fused(nz, ny, inp, pre, nrm, gain, wu, wd, cot, gi_out, gu_out, gg_out,
          nrm_v, cot_v, gain_v, st, st2, d_out, inp_v, inp_t, pre_v, dn, up, dp,
          part, gi_own, gi_send, gi_got, chain, y_send, y_got, acc,
          gacc, gx, gx2, gy, gy2, gz, loc, send, recv):
    nx, f32, bf16 = 2, jnp.float32, jnp.bfloat16
    rows, half = inp.shape
    nq, _, blk, cols = wd.shape
    ns = nz * ny
    width = 2 * half
    wide = nx * cols
    chunks = 4
    step = rows // chunks
    high = half // nq
    scaled = (rows * nz * ny * nx) ** (-0.5)

    me, core = lax.axis_index("fs"), lax.axis_index("tp")
    x, y, z = me % nx, (me // nx) % ny, me // (nx * ny)
    at_x = (me + 1 - 2 * x, core)
    at_y = (me + nx * (1 - 2 * y), core)
    at_up = (me + nx * ny, core)
    at_down = (me - nx * ny, core)
    at_core = (me, 1 - core)
    at_up2 = (me + 2 * nx * ny, core)
    at_down2 = (me - 2 * nx * ny, core)
    wire = Wire(send, recv, at_core)
    low_end, top_end = z > 0, z < nz - 1
    low2, top2 = z > 1, z < nz - 2
    reach = 1

    def place(zz, yy):
        return lax.rem(zz * ny + yy + core * nq, ns)

    local = {}

    def load(name, refs):
        index = len(local)
        local[name] = (lambda: pltpu.make_async_copy(*refs(), loc.at[index]))
        local[name]().start()

    def ready(name):
        local[name]().wait()

    load("nrm", lambda: (nrm, nrm_v))
    load("cot", lambda: (cot, cot_v))
    load("gain", lambda: (gain, gain_v))

    def own_dn(q, xx):
        start = place(z, y) * wide + xx * cols
        return dn.at[pl.ds(q * blk, blk), pl.ds(pl.multiple_of(start, cols), cols)]

    for q in range(nq):
        load(("dn", q), lambda q=q: (wd.at[q, x], own_dn(q, x)))
    for q in range(nq):
        load(("up", q), lambda q=q: (
            wu.at[pl.ds(q * high, high), :],
            up.at[pl.ds(q * high, high), pl.ds(pl.multiple_of(place(z, y) * blk, blk), blk)]))
    for q in range(nq):
        load(("pre", q), lambda q=q: (
            pre.at[:, pl.ds(pl.multiple_of((2 * q + x) * blk, blk), blk)], pre_v.at[0, q]))
    load("inp", lambda: (inp, inp_v.at[0]))

    barrier = pltpu.get_barrier_semaphore()
    peers = (
        (at_core, None), (at_x, None), (at_y, None), (at_up, top_end), (at_down, low_end),
    ) + (((at_up2, top2), (at_down2, low2)) if reach > 1 else ())
    for peer, live in peers:
        when(live, lambda: pl.semaphore_signal(
            barrier, inc=1, device_id=peer, device_id_type=MESH))
    count = 3
    for _, live in peers[3:]:
        count = count + live.astype(jnp.int32)
    pl.semaphore_wait(barrier, count)

    for q in range(nq):
        wire.put(lambda q=q: (wd.at[q, 1 - x], own_dn(q, x)), ("swap", q), at_x)

    ready("nrm")
    ready("cot")
    ready("gain")
    gacc[...] = jnp.zeros_like(gacc)
    tall = 32

    def stats(i, carry):
        r = pl.ds(pl.multiple_of(i * tall, tall), tall)
        n = nrm_v[r, :].astype(f32)
        u = cot_v[r, :].astype(f32) * gain_v[...]
        squares = jnp.sum(n * n, axis=1, keepdims=True)
        cross = jnp.sum(u * n, axis=1, keepdims=True)
        lane = lax.broadcasted_iota(jnp.int32, (tall, st.shape[1]), 1)
        st[r, :] = jnp.where(lane == 0, squares, cross)
        return carry

    lax.fori_loop(0, rows // tall, stats, 0)
    wire.put(lambda: (st, st2), "stats", at_core)

    def piece(name, j, zz, yy, part_of=0):
        buf, tile, w = gathers[name]
        first = (0, 0, tile // 2)[part_of]
        count = (tile, tile // 2, tile // 2)[part_of]
        return buf.at[pl.ds(j * tile + first, count),
                      pl.ds(pl.multiple_of(place(zz, yy) * w, w), w)]

    gathers = {"dn": (dn, blk, wide), "up": (up, high, blk)}
    odd = z % 2 == 1
    even = jnp.logical_not(odd)

    def over_y(name, j, zz, tag, live, halved=None):
        refs = lambda: (piece(name, j, zz, y),) * 2
        half_refs = lambda: (piece(name, j, zz, y, 1),) * 2
        key = (name, j, "y", tag)
        if halved is None:
            wire.put(refs, key, at_y, live, "y")
        else:
            wire.put(refs, key, at_y, both(live, jnp.logical_not(halved)), "y")
            wire.put(half_refs, key, at_y, both(live, halved), "y")

    def own(name, j):
        refs = lambda: (piece(name, j, z, y),) * 2
        wire.put(refs, (name, j, "u", 1), at_up, top_end)
        wire.put(refs, (name, j, "d", 1), at_down, low_end)
        over_y(name, j, z, "own", None)
        if reach > 1:
            wire.put(refs, (name, j, "u", 2), at_up2, top2)
            wire.put(refs, (name, j, "d", 2), at_down2, low2)

    def forward(name, j, k):
        for way, zz, live, device, ahead, halved in (
            ("u", z - k, z >= k, at_up, top_end, odd),
            ("d", z + k, z + k < nz, at_down, low_end, even),
        ):
            when(live, lambda: wire.got(piece(name, j, zz, y), (name, j, way, k)))
            if reach <= k < nz - 1:
                wire.put(lambda zz=zz: (piece(name, j, zz, y),) * 2, (name, j, way, k + 1),
                         device, both(live, ahead))
            over_y(name, j, zz, (way, k), live, halved if k == 1 else None)

    def side(name, j):
        wire.got(piece(name, j, z, 1 - y), (name, j, "y", "own"))
        refs = lambda: (piece(name, j, z, 1 - y, 2),) * 2
        wire.put(refs, (name, j, "side"), at_up, even)
        wire.put(refs, (name, j, "side"), at_down, odd)

    def arrived(name, j):
        for k in range(1, nz):
            for tag, zz, live, halved in (
                ("u", z - k, z >= k, odd), ("d", z + k, z + k < nz, even)
            ):
                key = (name, j, "y", (tag, k))
                if k == 1:
                    when(jnp.logical_and(live, halved), lambda: wire.got(
                        piece(name, j, zz, 1 - y, 1), key))
                    live = jnp.logical_and(live, jnp.logical_not(halved))
                when(live, lambda: wire.got(piece(name, j, zz, 1 - y), key))
        wire.got(piece(name, j, z + 1 - 2 * (z % 2), 1 - y, 2), (name, j, "side"))

    order = [("up", 0)] + [("dn", q) for q in range(nq)] + [("up", q) for q in range(1, nq)]

    def next_piece(p):
        if p < len(order):
            name, j = order[p]
            ready((name, j))
            if name == "dn":
                wire.got(own_dn(j, 1 - x), ("swap", j))
            own(name, j)

    next_piece(0)

    wire.got(st2, "stats")
    short = 16

    def norm(n_chunk):
        def rows_of(i, carry):
            r = pl.ds(pl.multiple_of(n_chunk * step + i * short, short), short)
            n = nrm_v[r, :].astype(f32)
            u = cot_v[r, :].astype(f32)
            both_sums = st[r, :] + st2[r, :]
            inv = lax.rsqrt(both_sums[:, 0:1] / width + norm_eps)
            cross = both_sums[:, 1:2] / width
            d = u * gain_v[...] * inv - n * (inv * inv * inv * cross)
            d_out[r, pl.ds(0, half)] = d.astype(bf16)
            g = u * n * inv
            gacc[...] += g[0:8] + g[8:16]
            return carry

        lax.fori_loop(0, step // short, rows_of, 0)

    def d_tile(t, n_chunk, h):
        return d_out.at[pl.ds(t * rows + n_chunk * step, step), pl.ds(h * half, half)]

    for n in range(chunks):
        norm(n)
        wire.put(lambda n=n: (d_tile(0, n, 0), d_tile(1, n, 0)), ("d_x", n), at_x)
        wire.put(lambda n=n: (d_tile(0, n, 0), d_tile(0, n, 1)), ("d_core", 0, n), at_core)

    gx[...] = jnp.sum(gacc[...], axis=0, keepdims=True)
    wire.put(lambda: (gx, gx2), "gain_x", at_x)
    wire.put(lambda: (inp, inp_v.at[1]), "inp", at_x)
    for q in range(nq):
        wire.put(lambda q=q: (
            pre.at[:, pl.ds(pl.multiple_of((2 * q + 1 - x) * blk, blk), blk)], pre_v.at[1, q]),
            ("pre", q), at_x)

    def turn(t):
        def cols_of(i, carry):
            c = pl.ds(pl.multiple_of(i * blk, blk), blk)
            for k in range(half // blk):
                inp_t[pl.ds(k * blk, blk), pl.ds(pl.multiple_of(t * rows + i * blk, blk), blk)] = (
                    inp_v[t, c, pl.ds(k * blk, blk)].T)
            return carry

        lax.fori_loop(0, rows // blk, cols_of, 0)

    def act(t, q):
        def rows_of(i, carry):
            r = pl.ds(pl.multiple_of(t * rows + i * blk, blk), blk)
            got = mm(d_out[r, :], dn[pl.ds(q * blk, blk), :])
            p = pre_v[t, q, pl.ds(pl.multiple_of(i * blk, blk), blk), :].astype(f32)
            dp[r, pl.ds(q * blk, blk)] = (got * 2.0 * jnp.maximum(p, 0.0)).astype(bf16)
            return carry

        lax.fori_loop(0, rows // blk, rows_of, 0)
        tile = lambda s: dp.at[pl.ds(t * rows, rows), pl.ds((s * nq + q) * blk, blk)]
        wire.put(lambda: (tile(0), tile(1)), ("dp", t, q), at_core)

    def relay(p, k):
        forward(*order[p], k)
        if k == 1:
            side(*order[p])
            next_piece(p + 3)

    def d_back(n):
        wire.got(d_tile(1, n, 0), ("d_x", n))
        wire.put(lambda: (d_tile(1, n, 0), d_tile(1, n, 1)), ("d_core", 1, n), at_core)

    def act_own(q):
        if q == 0:
            for n in range(chunks):
                wire.got(d_tile(0, n, 1), ("d_core", 0, n))
        ready(("pre", q))
        arrived("dn", q)
        act(0, q)

    def act_far(q):
        if q == 0:
            for n in range(chunks):
                wire.got(d_tile(1, n, 1), ("d_core", 1, n))
        wire.got(pre_v.at[1, q], ("pre", q))
        act(1, q)

    def back(r):
        def rows_of(i, carry):
            k = pl.ds(pl.multiple_of(i * blk, blk), blk)
            w = up[pl.ds(r * high, high), :]
            far = mm(dp[pl.ds(pl.multiple_of(rows + i * blk, blk), blk), :], w)
            gi_send[r, k, :] = far.astype(bf16)
            return carry

        def rows_own(i, carry):
            k = pl.ds(pl.multiple_of(i * blk, blk), blk)
            w = up[pl.ds(r * high, high), :]
            gi_own[r, k, :] = mm(dp[k, :], w)
            return carry

        lax.fori_loop(0, rows // blk, rows_of, 0)
        wire.put(lambda: (gi_send.at[r], gi_got.at[r]), ("gi", r), at_x)
        lax.fori_loop(0, rows // blk, rows_own, 0)

    def grads(q):
        for t in range(nx):
            wire.got(dp.at[pl.ds(t * rows, rows), pl.ds((nq + q) * blk, blk)], ("dp", t, q))
        for j in (q, nq + q):
            for r in range(nq):
                part[r, j] = lax.dot_general(
                    inp_t[pl.ds(r * high, high), :], dp[:, pl.ds(j * blk, blk)],
                    (((1,), (0,)), ((), ())), preferred_element_type=f32)

    def goals(q):
        return [divmod(b, ny) for b in (q, nq + q)]

    def first_y(r):
        return r >= split

    def to_y(q, r):
        for goal, column in goals(q):
            live = y != column

            @pl.when(live)
            def _():
                y_send[r, goal] = part[r, place(goal, column)].astype(bf16)

            wire.put(lambda goal=goal: (y_send.at[r, goal], y_got.at[r, goal]),
                     ("y", r, goal), at_y, live)

    def link(q, r, level):
        for goal, column in goals(q):
            for kind in range(2):
                at = level if kind == 0 else nz - 1 - level
                if at >= goal if kind == 0 else at <= goal:
                    continue
                slot = chain.at[kind, r, goal, column]
                key = ("sum", kind, r, goal, column)
                live = z == at
                if first_y(r):
                    live = jnp.logical_and(live, y == column)

                @pl.when(live)
                def _():
                    value = part[r, place(goal, column)]
                    if first_y(r):
                        wire.got(y_got.at[r, goal], ("y", r, goal))
                        value = value + y_got[r, goal].astype(f32)
                    if level > 0:
                        wire.got(slot, key)
                        value = value + slot[...].astype(f32)
                    slot[...] = value.astype(bf16)

                wire.put(lambda slot=slot: (slot, slot), key,
                         at_up if kind == 0 else at_down, live)

    def settle(q, r):
        for goal, column in goals(q):
            live = z == goal
            if first_y(r):
                live = jnp.logical_and(live, y == column)

            @pl.when(live)
            def _():
                value = part[r, place(goal, column)]
                if first_y(r):
                    wire.got(y_got.at[r, goal], ("y", r, goal))
                    value = value + y_got[r, goal].astype(f32)
                for kind in range(2):
                    if goal != (0, nz - 1)[kind]:
                        slot = chain.at[kind, r, goal, column]
                        wire.got(slot, ("sum", kind, r, goal, column))
                        value = value + slot[...].astype(f32)
                if first_y(r):
                    gu_out[pl.ds(r * high, high), :] = value * scaled
                else:
                    acc[r] = value

            if not first_y(r):
                away = jnp.logical_and(live, y != column)

                @pl.when(away)
                def _():
                    y_send[r, 0] = acc[r].astype(bf16)

                @pl.when(jnp.logical_and(live, y == column))
                def _():
                    gu_out[pl.ds(r * high, high), :] = acc[r]

                wire.put(lambda: (y_send.at[r, 0], y_got.at[r, 0]), ("y", r), at_y, away)

    split = nq // 2
    first = list(range(split))
    later = list(range(split, nq))

    def step_of(rows_set, q, level):
        for r in rows_set:
            if level < nz - 1:
                link(q, r, level)
            else:
                settle(q, r)

    def z_step(q, level):
        step_of(first, q, level)

    def y_step(q, level):
        step_of(later, q, level)

    def gain_over_y():
        wire.got(gx2, "gain_x")
        gy[...] = gx[...] + gx2[...]
        wire.put(lambda: (gy, gy2), "gain_y", at_y)

    def gain_over_z():
        wire.got(gy2, "gain_y")
        gz[z] = gy[...] + gy2[...]
        wire.put(lambda: (gz.at[z], gz.at[z]), ("gain", "u", 1), at_up, top_end)
        wire.put(lambda: (gz.at[z], gz.at[z]), ("gain", "d", 1), at_down, low_end)

    def over_rows(q):
        for r in later:
            to_y(q, r)

    def gain_relay(k):
        for key, slot, live, device, ahead in (
            ("u", z - k, z >= k, at_up, top_end), ("d", z + k, z + k < nz, at_down, low_end)
        ):
            when(live, lambda: wire.got(gz.at[slot], ("gain", key, k)))
            if k + 1 < nz:
                wire.put(lambda slot=slot: (gz.at[slot], gz.at[slot]), ("gain", key, k + 1),
                         device, both(live, ahead))

    for p in range(1, 3):
        next_piece(p)
    relay(0, 1)
    relay(1, 1)
    relay(0, 2)
    relay(2, 1)
    d_back(0)
    relay(1, 2)
    relay(2, 2)
    relay(3, 1)
    relay(0, 3)
    relay(1, 3)
    relay(2, 3)
    d_back(1)
    ready("inp")
    turn(0)
    d_back(2)
    d_back(3)
    gain_over_y()
    relay(4, 1)
    act_own(0)
    relay(3, 2)
    relay(4, 2)
    relay(5, 1)
    wire.got(inp_v.at[1], "inp")
    turn(1)
    act_own(1)
    relay(6, 1)
    gain_over_z()
    act_far(0)
    grads(0)
    relay(3, 3)
    z_step(0, 0)
    act_far(1)
    relay(4, 3)
    grads(1)
    z_step(1, 0)
    act_own(2)
    act_far(2)
    relay(5, 2)
    relay(6, 2)
    relay(7, 1)
    grads(2)
    gain_relay(1)
    z_step(2, 0)
    relay(5, 3)
    z_step(0, 1)
    relay(6, 3)
    act_own(3)
    act_far(3)
    grads(3)
    over_rows(3)
    over_rows(2)
    over_rows(0)
    z_step(0, 2)
    z_step(3, 0)
    arrived("up", 1)
    back(1)
    over_rows(1)
    relay(7, 2)
    gain_relay(2)
    z_step(1, 1)
    relay(7, 3)
    y_step(3, 0)
    y_step(2, 0)
    arrived("up", 2)
    back(2)
    y_step(0, 0)
    z_step(2, 1)
    y_step(1, 0)
    z_step(2, 2)
    z_step(3, 1)
    z_step(1, 2)
    z_step(1, 3)
    z_step(3, 2)
    z_step(3, 3)
    y_step(3, 1)
    gain_relay(3)
    y_step(2, 1)
    arrived("up", 0)
    back(0)
    arrived("up", 3)
    back(3)
    z_step(2, 3)
    y_step(1, 1)
    y_step(0, 1)
    y_step(3, 2)
    y_step(0, 2)
    z_step(0, 3)
    y_step(1, 2)
    y_step(2, 2)
    y_step(2, 3)
    y_step(3, 3)
    y_step(0, 3)
    y_step(1, 3)
    total = gz[0]
    for k in range(1, nz):
        total = total + gz[k]
    gg_out[...] = total * scaled
    for r in range(nq):
        wire.got(gi_got.at[r], ("gi", r))
        gi_out[:, pl.ds(r * high, high)] = (gi_own[r] + gi_got[r].astype(f32)).astype(bf16)
    for r in first:
        wire.got(y_got.at[r, 0], ("y", r))
        tile = pl.ds(r * high, high)
        gu_out[tile, :] = (gu_out[tile, :] + y_got[r, 0].astype(f32)) * scaled
    wire.drain()


def kernel_step(fs, tp, inputs, hidden_pre, norm_input, out_gain, w_up, w_down, cotangent):
    nx = ny = 2
    nz = fs // (nx * ny)
    rows, half = inputs.shape
    blk, cols = w_up.shape[1], w_down.shape[1]
    nq = nz * ny // tp
    ns, high = nz * ny, half // nq
    hid = nq * blk
    f32, bf16 = jnp.float32, jnp.bfloat16
    v = pltpu.VMEM
    scratch = [
        v((rows, half), bf16), v((rows, half), bf16), v((1, half), f32),
        v((rows, 128), f32), v((rows, 128), f32),
        v((nx * rows, 2 * half), bf16),
        v((nx, rows, half), bf16), v((half, nx * rows), bf16),
        v((nx, nq, rows, blk), bf16),
        v((hid, 2 * half), bf16), v((half, ns * blk), bf16), v((nx * rows, ns * blk), bf16),
        v((nq, ns, high, blk), f32),
        v((nq, rows, high), f32), v((nq, rows, high), bf16), v((nq, rows, high), bf16),
        v((2, nq, nz, ny, high, blk), bf16),
        v((nq, nz, high, blk), bf16), v((nq, nz, high, blk), bf16),
        v((nq // 2, high, blk), f32),
        v((8, half), f32),
        v((1, half), f32), v((1, half), f32), v((1, half), f32), v((1, half), f32),
        v((nz, 1, half), f32),
        pltpu.SemaphoreType.DMA((3 + 3 * nq + 1,)),
        pltpu.SemaphoreType.DMA((SEMS,)), pltpu.SemaphoreType.DMA((SEMS,)),
    ]
    flops = 3 * 2 * nx * rows * 2 * half * hid
    shapes = ((rows, half), bf16), ((half, blk), f32), ((1, half), f32)
    results = pl.pallas_call(
        functools.partial(fused, nz, ny),
        out_shape=tuple(v(*shape) for shape in shapes),
        in_specs=[pl.BlockSpec(memory_space=pl.ANY)] * 7,
        out_specs=(pl.BlockSpec(memory_space=pltpu.VMEM),) * 3,
        scratch_shapes=scratch,
        compiler_params=pltpu.CompilerParams(
            collective_id=0, has_side_effects=True, vmem_limit_bytes=60 << 20
        ),
        cost_estimate=pl.CostEstimate(flops=flops, bytes_accessed=1 << 24, transcendentals=0),
        name="layer_backward",
    )(
        inputs, hidden_pre, norm_input, out_gain.reshape(1, half), w_up,
        w_down.reshape(nq, nx, blk, cols), cotangent,
    )
    grad_input, grad_up, grad_gain = results
    return grad_input, grad_up, grad_gain.reshape(half)


def in_kernel(*args):
    return kernel_step(lax.axis_size("fs"), lax.axis_size("tp"), *args)


def solution(mesh):
    placed = (
        P("fs", "tp"),
        P("fs", "tp"),
        P("fs", "tp"),
        P("tp"),
        P("tp", "fs"),
        P("tp", "fs"),
        P("fs", "tp"),
    )
    fs, tp = mesh.shape["fs"], mesh.shape["tp"]
    out_specs = (P("fs", "tp"), P("tp", "fs"), P("tp"))

    def solve(*args):
        up, down = args[4].shape, args[5].shape
        if tp == 2 and fs % 8 == 0 and up[1] // fs % 256 == 0 and down[1] // fs % 128 == 0:
            return jax.shard_map(
                in_kernel, mesh=mesh, in_specs=placed, out_specs=out_specs, check_vma=False
            )(*args)
        return permuted(*args)

    step = jax.shard_map(
        on_device,
        mesh=mesh,
        in_specs=placed,
        out_specs=(P("fs", "tp"), P("tp", "fs"), P("tp")),
        check_vma=False,
    )
    permuted = step
    return solve
```

```python
import functools

import jax
import jax.numpy as jnp
from jax import lax
from jax.experimental import pallas as pl
from jax.experimental.pallas import tpu as pltpu
from jax.sharding import PartitionSpec as P


norm_eps = 1e-06
MESH = pl.DeviceIdType.MESH
SENDS = 170
RECVS = 160
PLAN_STEPS = 4
FULL_SIDE = ()
Y_FIRST = ((0, 3), (1, 3), (2, 2), (2, 3), (3, 0), (3, 3))
X_ORDER = (("pre", 0), ("inp", 0), ("inp", 2), ("pre", 2), ("inp", 1), ("pre", 1), ("pre", 3), ("inp", 3))


def trade(x, axis, mask):
    if mask == 0:
        return x
    return lax.ppermute(x, axis, [(i, i ^ mask) for i in range(lax.axis_size(axis))])


def total(x, axis):
    step = 1
    while step < lax.axis_size(axis):
        x = x + trade(x, axis, step)
        step *= 2
    return x


def masks_of(n):
    masks = [1 << i for i in range(n.bit_length() - 1)]
    return (masks, masks[::-1])


def halves(x):
    rows = x.shape[0] // 2
    return (x[:rows], x[rows:])


def gather_near(x, near_n):
    parts = []
    for part, masks in zip(halves(x), masks_of(near_n)):
        held = {0: part}
        for mask in masks:
            held.update({k ^ mask: trade(v, "fs", mask) for k, v in list(held.items())})
        parts.append(held)
    return parts


def scatter_near(pieces, near_n):
    sums = []
    for side, masks in enumerate(masks_of(near_n)):
        held = {k: halves(v)[side] for k, v in pieces.items()}
        for mask in masks:
            sent = {k: held.pop(k) for k in list(held) if k & mask}
            for k, v in sent.items():
                came = trade(v.astype(jnp.bfloat16), "fs", mask).astype(jnp.float32)
                held[k ^ mask] = held[k ^ mask] + came
        sums.append(held[0])
    return jnp.concatenate(sums, axis=0)


def tree(x, n, unit):
    terms = [trade(x, "fs", k * unit) for k in range(n)]
    while len(terms) > 1:
        terms = [a + b for a, b in zip(terms[::2], terms[1::2])]
    return terms[0]


def pick(stack, index):
    return lax.dynamic_index_in_dim(stack, index, 0, keepdims=False)


def dot(a, b, dim):
    return lax.dot_general(
        a, b, (((dim,), (dim,)), ((), ())), preferred_element_type=jnp.float32
    )


def on_device(inputs, hidden_pre, norm_input, out_gain, w_up, w_down, cotangent):
    fs, tp = lax.axis_size("fs"), lax.axis_size("tp")
    near_n = 1
    while 4 * near_n * near_n <= fs:
        near_n *= 2
    far_n = fs // near_n
    per = far_n // tp
    me, core = lax.axis_index("fs"), lax.axis_index("tp")
    far, near = me // near_n, me % near_n
    rows = inputs.shape[0]
    width = inputs.shape[1] * tp
    scaled = (rows * fs) ** (-0.5)
    block = w_up.shape[1]
    cols = w_down.shape[1]

    down_rows = w_down.reshape(per, near_n, block, cols)
    asked = [
        lax.dynamic_index_in_dim(down_rows, near ^ k, 1, keepdims=False).reshape(per * block, cols)
        for k in range(near_n)
    ]
    arrived = [trade(x, "fs", k) for k, x in enumerate(asked)]
    arrived = jnp.stack(arrived)
    down_near = jnp.concatenate([pick(arrived, near ^ i) for i in range(near_n)], axis=1)
    down_far = [trade(down_near, "fs", k * near_n) for k in range(far_n)]
    up_far = [trade(w_up, "fs", k * near_n) for k in range(far_n)]
    up_far = jnp.stack(up_far)
    down_far = jnp.stack(down_far)
    down, up = [], []
    for t in range(tp):
        places = [((core ^ t) * per + j) ^ far for j in range(per)]
        down.append(jnp.concatenate([pick(down_far, i) for i in places], axis=1))
        up.append(jnp.concatenate([pick(up_far, i) for i in places], axis=1))

    asked = [
        jnp.concatenate(
            [
                lax.dynamic_slice_in_dim(
                    hidden_pre, (j * near_n + (near ^ k)) * block, block, axis=1
                )
                for j in range(per)
            ],
            axis=1,
        )
        for k in range(near_n)
    ]
    pre = [trade(x, "fs", k) for k, x in enumerate(asked)]

    normed = norm_input.astype(jnp.float32)
    upstream = cotangent.astype(jnp.float32)
    weighted = upstream * out_gain
    sums = total(
        jnp.stack([jnp.sum(normed * normed, axis=1), jnp.sum(weighted * normed, axis=1)]), "tp"
    )
    inv_rms = lax.rsqrt(sums[0] / width + norm_eps)[:, None]
    cross_mean = (sums[1] / width)[:, None]
    d_out = (weighted * inv_rms - normed * inv_rms * inv_rms * inv_rms * cross_mean).astype(
        jnp.bfloat16
    )
    gain = jnp.sum(upstream * normed * inv_rms, axis=0) * scaled
    gain = tree(gain, near_n, 1)
    grad_gain = tree(gain, far_n, near_n)

    d_outs = gather_near(d_out, near_n)
    tokens = gather_near(inputs, near_n)
    d_pres, partial = [], {}
    for k in range(near_n):
        d_out_k = jnp.concatenate([d_outs[0][k], d_outs[1][k]], axis=0)
        d_out_k = [trade(d_out_k, "tp", t) for t in range(tp)]
        d_act = sum(dot(d_out_k[t], down[t], 1) for t in range(tp))
        d_pre = (d_act * 2.0 * jax.nn.relu(pre[k].astype(jnp.float32))).astype(jnp.bfloat16)
        d_pres.append([trade(d_pre, "tp", t) for t in range(tp)])
        partial[k] = sum(dot(d_pres[k][t], up[t], 1) for t in range(tp))
    grad_input = scatter_near(partial, near_n)

    all_pres = [
        jnp.concatenate([d_pres[k][t] for k in range(near_n)], axis=0) for t in range(tp)
    ]
    all_tokens = jnp.concatenate([side[k] for k in range(near_n) for side in tokens], axis=0)
    sums_up = [dot(x, all_tokens, 0) for x in all_pres]
    sums_up = jnp.concatenate(sums_up, axis=0).reshape(
        far_n, block, inputs.shape[1]
    )
    grad_up = 0.0
    for k in range(far_n):
        goal = far ^ k
        mine = pick(sums_up, (core ^ (goal // per)) * per + goal % per)
        if k:
            mine = trade(mine.astype(jnp.bfloat16), "fs", k * near_n).astype(jnp.float32)
        grad_up = grad_up + mine
    return (grad_input.astype(jnp.bfloat16), (grad_up * scaled).T, grad_gain)


def mm(a, b):
    return lax.dot_general(a, b, (((1,), (1,)), ((), ())), preferred_element_type=jnp.float32)


class Wire:
    def __init__(self, send, recv, other, nz):
        self.send, self.recv, self.other, self.nz = send, recv, other, nz
        self.sent, self.came, self.pending = {}, {}, []

    def arrives(self, key):
        *head, way, k = key if isinstance(key, tuple) else (key, None, None)
        if key[0] == "sum":
            kind, r, goal, column = key[1:]
            return "sum", r, goal + 1 - kind, column
        if way == "d":
            return *head, "u", self.nz - k
        if way == "y" and k[0] == "d":
            return *head, "y", ("u", self.nz - k[1])
        return key

    def departs(self, key):
        if key[0] == "sum":
            return "sum", *key[2:]
        if isinstance(key, tuple) and key[-2] == "d":
            return key if key[-1] < self.nz - 1 else (*key[:-2], "u", key[-1])
        return self.arrives(key)

    def at(self, sems, names, key):
        index = names.setdefault(key, len(names))
        assert index < sems.shape[0], "semaphores"
        return sems.at[index]

    def put(self, refs, key, device, live=None):
        out = self.at(self.send, self.sent, self.departs(key))
        arrival = self.at(self.recv, self.came, self.arrives(key))

        def copy():
            source, target = refs()
            return pltpu.make_async_remote_copy(
                src_ref=source, dst_ref=target, send_sem=out, recv_sem=arrival,
                device_id=device, device_id_type=MESH,
            )

        when(live, lambda: copy().start())
        self.pending.append((copy, live))

    def got(self, ref, key):
        pltpu.make_async_remote_copy(
            src_ref=ref, dst_ref=ref, send_sem=self.send.at[0],
            recv_sem=self.at(self.recv, self.came, self.arrives(key)),
            device_id=self.other, device_id_type=MESH,
        ).wait_recv()

    def drain(self):
        for copy, live in self.pending:
            when(live, lambda: copy().wait_send())
        self.pending = []


def when(live, body):
    if live is None:
        body()
    else:
        pl.when(live)(body)


def both(a, b):
    return a if b is None else b if a is None else jnp.logical_and(a, b)


def fused(nz, ny, inp, pre, nrm, gain, wu, wd, cot, gi_out, gu_out, gg_out,
          nrm_v, cot_v, gain_v, st, st2, d_out, inp_v, inp_t, pre_v, dn, up, dp,
          part, gi_own, gi_send, gi_got, chain, y_send, y_got,
          tot_send, tot_got, acc, gacc, gx, gx2, gy, gy2, gz, loc, send, recv):
    nx, f32, bf16 = 2, jnp.float32, jnp.bfloat16
    rows, half = inp.shape
    nq, _, blk, cols = wd.shape
    ns = nz * ny
    width = 2 * half
    wide = nx * cols
    chunks = 4
    step = rows // chunks
    high = half // nq
    scaled = (rows * nz * ny * nx) ** (-0.5)

    me, core = lax.axis_index("fs"), lax.axis_index("tp")
    x, y, z = me % nx, (me // nx) % ny, me // (nx * ny)
    at_x = (me + 1 - 2 * x, core)
    at_y = (me + nx * (1 - 2 * y), core)
    at_up = (me + nx * ny, core)
    at_down = (me - nx * ny, core)
    at_core = (me, 1 - core)
    wire = Wire(send, recv, at_core, nz)
    low_end, top_end = z > 0, z < nz - 1

    def place(zz, yy):
        return lax.rem(zz * ny + yy + core * nq, ns)

    local = {}

    def load(name, refs):
        index = len(local)
        local[name] = (lambda: pltpu.make_async_copy(*refs(), loc.at[index]))
        local[name]().start()

    def ready(name):
        local[name]().wait()

    load("nrm", lambda: (nrm, nrm_v))
    load("cot", lambda: (cot, cot_v))
    load("gain", lambda: (gain, gain_v))

    def own_dn(q, xx):
        start = place(z, y) * wide + xx * cols
        return dn.at[pl.ds(q * blk, blk), pl.ds(pl.multiple_of(start, cols), cols)]

    for q in range(nq):
        load(("dn", q), lambda q=q: (wd.at[q, x], own_dn(q, x)))
    for q in range(nq):
        load(("up", q), lambda q=q: (
            wu.at[pl.ds(q * high, high), :],
            up.at[pl.ds(q * high, high), pl.ds(pl.multiple_of(place(z, y) * blk, blk), blk)]))
    for q in range(nq):
        load(("pre", q), lambda q=q: (
            pre.at[:, pl.ds(pl.multiple_of((2 * q + x) * blk, blk), blk)], pre_v.at[0, q]))
    load("inp", lambda: (inp, inp_v.at[0]))

    barrier = pltpu.get_barrier_semaphore()
    peers = (
        (at_core, None), (at_x, None), (at_y, None), (at_up, top_end), (at_down, low_end),
    )
    for peer, live in peers:
        when(live, lambda: pl.semaphore_signal(
            barrier, inc=1, device_id=peer, device_id_type=MESH))
    count = 3
    for _, live in peers[3:]:
        count = count + live.astype(jnp.int32)

    ready("nrm")
    ready("cot")
    ready("gain")
    gacc[...] = jnp.zeros_like(gacc)
    tall = 32

    def stats(i, carry):
        r = pl.ds(pl.multiple_of(i * tall, tall), tall)
        n = nrm_v[r, :].astype(f32)
        u = cot_v[r, :].astype(f32) * gain_v[...]
        squares = jnp.sum(n * n, axis=1, keepdims=True)
        cross = jnp.sum(u * n, axis=1, keepdims=True)
        lane = lax.broadcasted_iota(jnp.int32, (tall, st.shape[1]), 1)
        st[r, :] = jnp.where(lane == 0, squares, cross)
        return carry

    lax.fori_loop(0, rows // tall, stats, 0)

    pl.semaphore_wait(barrier, count)

    wire.put(lambda: (st, st2), "stats", at_core)
    for q in range(nq):
        wire.put(lambda q=q: (wd.at[q, 1 - x], own_dn(q, x)), ("swap", q), at_x)


    def piece(name, j, zz, yy, part_of=0):
        buf, tile, w = gathers[name]
        first = (0, 0, tile // 2)[part_of]
        count = (tile, tile // 2, tile // 2)[part_of]
        return buf.at[pl.ds(j * tile + first, count),
                      pl.ds(pl.multiple_of(place(zz, yy) * w, w), w)]

    gathers = {"dn": (dn, blk, wide), "up": (up, high, blk)}
    odd = z % 2 == 1
    even = jnp.logical_not(odd)

    def over_y(name, j, zz, tag, live, halved=None):
        refs = lambda: (piece(name, j, zz, y),) * 2
        half_refs = lambda: (piece(name, j, zz, y, 1),) * 2
        key = (name, j, "y", tag)
        if halved is None:
            wire.put(refs, key, at_y, live)
        else:
            wire.put(refs, key, at_y, both(live, jnp.logical_not(halved)))
            if (name, j) not in FULL_SIDE:
                wire.put(half_refs, key, at_y, both(live, halved))

    def own(name, j):
        refs = lambda: (piece(name, j, z, y),) * 2
        wire.put(refs, (name, j, "u", 1), at_up, top_end)
        wire.put(refs, (name, j, "d", 1), at_down, low_end)
        over_y(name, j, z, "own", None)

    def forward(name, j, k):
        for way, zz, live, device, ahead, halved in (
            ("u", z - k, z >= k, at_up, top_end, odd),
            ("d", z + k, z + k < nz, at_down, low_end, even),
        ):
            when(live, lambda: wire.got(piece(name, j, zz, y), (name, j, way, k)))
            if k < nz - 1:
                wire.put(lambda zz=zz: (piece(name, j, zz, y),) * 2, (name, j, way, k + 1),
                         device, both(live, ahead))
            over_y(name, j, zz, (way, k), live, halved if k == 1 else None)

    def side(name, j):
        wire.got(piece(name, j, z, 1 - y), (name, j, "y", "own"))
        share = 0 if (name, j) in FULL_SIDE else 2
        refs = lambda: (piece(name, j, z, 1 - y, share),) * 2
        wire.put(refs, (name, j, "side"), at_up, even)
        wire.put(refs, (name, j, "side"), at_down, odd)

    def arrived(name, j):
        for k in range(1, nz):
            for tag, zz, live, halved in (
                ("u", z - k, z >= k, odd), ("d", z + k, z + k < nz, even)
            ):
                key = (name, j, "y", (tag, k))
                if k == 1:
                    if (name, j) not in FULL_SIDE:
                        when(jnp.logical_and(live, halved), lambda: wire.got(
                            piece(name, j, zz, 1 - y, 1), key))
                    live = jnp.logical_and(live, jnp.logical_not(halved))
                when(live, lambda: wire.got(piece(name, j, zz, 1 - y), key))
        share = 0 if (name, j) in FULL_SIDE else 2
        wire.got(piece(name, j, z + 1 - 2 * (z % 2), 1 - y, share), (name, j, "side"))

    def send_piece(name, j):
        ready((name, j))
        if name == "dn":
            wire.got(own_dn(j, 1 - x), ("swap", j))
        own(name, j)

    send_piece("up", 0)

    wire.got(st2, "stats")
    short = 16

    def norm(n_chunk):
        def rows_of(i, carry):
            r = pl.ds(pl.multiple_of(n_chunk * step + i * short, short), short)
            n = nrm_v[r, :].astype(f32)
            u = cot_v[r, :].astype(f32)
            both_sums = st[r, :] + st2[r, :]
            inv = lax.rsqrt(both_sums[:, 0:1] / width + norm_eps)
            cross = both_sums[:, 1:2] / width
            d = u * gain_v[...] * inv - n * (inv * inv * inv * cross)
            d_out[r, pl.ds(0, half)] = d.astype(bf16)
            g = u * n * inv
            gacc[...] += g[0:8] + g[8:16]
            return carry

        lax.fori_loop(0, step // short, rows_of, 0)

    def d_tile(t, n_chunk, h):
        return d_out.at[pl.ds(t * rows + n_chunk * step, step), pl.ds(h * half, half)]

    def send_d(n):
        norm(n)
        wire.put(lambda: (d_tile(0, n, 0), d_tile(1, n, 0)), ("d_x", n), at_x)
        wire.put(lambda: (d_tile(0, n, 0), d_tile(0, n, 1)), ("d_core", 0, n), at_core)

    def send_x():
        gx[...] = jnp.sum(gacc[...], axis=0, keepdims=True)
        wire.put(lambda: (gx, gx2), "gain_x", at_x)
        for kind, q in X_ORDER:
            if kind == "inp":
                tile = pl.ds(q * high, high)
                wire.put(lambda tile=tile: (inp.at[:, tile], inp_v.at[1, :, tile]),
                         ("inp", q), at_x)
            else:
                wire.put(lambda q=q: (
                    pre.at[:, pl.ds(pl.multiple_of((2 * q + 1 - x) * blk, blk), blk)],
                    pre_v.at[1, q]), ("pre", q), at_x)

    def turn(t, r):
        tile = pl.ds(r * high, high)
        if t == 0:
            if r == 0:
                ready("inp")
        else:
            wire.got(inp_v.at[1, :, tile], ("inp", r))

        def rows_of(i, carry):
            tokens = pl.ds(pl.multiple_of(i * blk, blk), blk)
            inp_t[tile, pl.ds(pl.multiple_of(t * rows + i * blk, blk), blk)] = (
                inp_v[t, tokens, tile].T)
            return carry

        lax.fori_loop(0, rows // blk, rows_of, 0)

    def act(t, q):
        def rows_of(i, carry):
            r = pl.ds(pl.multiple_of(t * rows + i * blk, blk), blk)
            got = mm(d_out[r, :], dn[pl.ds(q * blk, blk), :])
            p = pre_v[t, q, pl.ds(pl.multiple_of(i * blk, blk), blk), :].astype(f32)
            dp[r, pl.ds(q * blk, blk)] = (got * 2.0 * jnp.maximum(p, 0.0)).astype(bf16)
            return carry

        lax.fori_loop(0, rows // blk, rows_of, 0)
        tile = lambda s: dp.at[pl.ds(t * rows, rows), pl.ds((s * nq + q) * blk, blk)]
        wire.put(lambda: (tile(0), tile(1)), ("dp", t, q), at_core)

    def d_back(n):
        wire.got(d_tile(1, n, 0), ("d_x", n))
        wire.put(lambda: (d_tile(1, n, 0), d_tile(1, n, 1)), ("d_core", 1, n), at_core)

    def act_own(q):
        if q == 0:
            for n in range(chunks):
                wire.got(d_tile(0, n, 1), ("d_core", 0, n))
        ready(("pre", q))
        arrived("dn", q)
        act(0, q)

    def act_far(q):
        if q == 0:
            for n in range(chunks):
                wire.got(d_tile(1, n, 1), ("d_core", 1, n))
        wire.got(pre_v.at[1, q], ("pre", q))
        act(1, q)

    def back_far(r):
        arrived("up", r)

        def rows_of(i, carry):
            k = pl.ds(pl.multiple_of(i * blk, blk), blk)
            w = up[pl.ds(r * high, high), :]
            far = mm(dp[pl.ds(pl.multiple_of(rows + i * blk, blk), blk), :], w)
            gi_send[r, k, :] = far.astype(bf16)
            return carry

        lax.fori_loop(0, rows // blk, rows_of, 0)
        wire.put(lambda: (gi_send.at[r], gi_got.at[r]), ("gi", r), at_x)

    def back_own(r):
        def rows_of(i, carry):
            k = pl.ds(pl.multiple_of(i * blk, blk), blk)
            w = up[pl.ds(r * high, high), :]
            gi_own[r, k, :] = mm(dp[k, :], w)
            return carry

        lax.fori_loop(0, rows // blk, rows_of, 0)

    def have_pre(q):
        for t in range(nx):
            wire.got(dp.at[pl.ds(t * rows, rows), pl.ds((nq + q) * blk, blk)], ("dp", t, q))

    def grads(q, r):
        for j in (q, nq + q):
            part[r, j] = lax.dot_general(
                inp_t[pl.ds(r * high, high), :], dp[:, pl.ds(j * blk, blk)],
                (((1,), (0,)), ((), ())), preferred_element_type=f32)

    def goals(q):
        return [divmod(b, ny) for b in (q, nq + q)]

    def first_y(q, r):
        return (q, r) in Y_FIRST

    def to_y(q, r):
        if not first_y(q, r):
            return
        for goal, column in goals(q):
            live = y != column

            @pl.when(live)
            def _():
                y_send[r, goal] = part[r, place(goal, column)].astype(bf16)

            wire.put(lambda goal=goal: (y_send.at[r, goal], y_got.at[r, goal]),
                     ("y", r, goal), at_y, live)

    def link(q, r, level):
        for goal, column in goals(q):
            for kind in range(2):
                at = level if kind == 0 else nz - 1 - level
                if at >= goal if kind == 0 else at <= goal:
                    continue
                slot = chain.at[kind, r, goal, column]
                key = ("sum", kind, r, goal, column)
                live = z == at
                if first_y(q, r):
                    live = jnp.logical_and(live, y == column)

                @pl.when(live)
                def _():
                    value = part[r, place(goal, column)]
                    if first_y(q, r):
                        wire.got(y_got.at[r, goal], ("y", r, goal))
                        value = value + y_got[r, goal].astype(f32)
                    if level > 0:
                        wire.got(slot, key)
                        value = value + slot[...].astype(f32)
                    slot[...] = value.astype(bf16)

                wire.put(lambda slot=slot: (slot, slot), key,
                         at_up if kind == 0 else at_down, live)

    def settle(q, r):
        for goal, column in goals(q):
            live = z == goal
            if first_y(q, r):
                live = jnp.logical_and(live, y == column)

            @pl.when(live)
            def _():
                value = part[r, place(goal, column)]
                if first_y(q, r):
                    wire.got(y_got.at[r, goal], ("y", r, goal))
                    value = value + y_got[r, goal].astype(f32)
                for kind in range(2):
                    if goal != (0, nz - 1)[kind]:
                        slot = chain.at[kind, r, goal, column]
                        wire.got(slot, ("sum", kind, r, goal, column))
                        value = value + slot[...].astype(f32)
                if first_y(q, r):
                    gu_out[pl.ds(r * high, high), :] = value * scaled
                else:
                    acc[r] = value

            if not first_y(q, r):
                away = jnp.logical_and(live, y != column)

                @pl.when(away)
                def _():
                    tot_send[r] = acc[r].astype(bf16)

                @pl.when(jnp.logical_and(live, y == column))
                def _():
                    gu_out[pl.ds(r * high, high), :] = acc[r]

                wire.put(lambda: (tot_send.at[r], tot_got.at[r]), ("total", r), at_y, away)

    def sum_step(q, r, level):
        if level < nz - 1:
            link(q, r, level)
        else:
            settle(q, r)

    def gain_over_y():
        wire.got(gx2, "gain_x")
        gy[...] = gx[...] + gx2[...]
        wire.put(lambda: (gy, gy2), "gain_y", at_y)

    def gain_over_z():
        wire.got(gy2, "gain_y")
        gz[z] = gy[...] + gy2[...]
        wire.put(lambda: (gz.at[z], gz.at[z]), ("gain", "u", 1), at_up, top_end)
        wire.put(lambda: (gz.at[z], gz.at[z]), ("gain", "d", 1), at_down, low_end)

    def gain_relay(k):
        for key, slot, live, device, ahead in (
            ("u", z - k, z >= k, at_up, top_end), ("d", z + k, z + k < nz, at_down, low_end)
        ):
            when(live, lambda: wire.got(gz.at[slot], ("gain", key, k)))
            if k + 1 < nz:
                wire.put(lambda slot=slot: (gz.at[slot], gz.at[slot]), ("gain", key, k + 1),
                         device, both(live, ahead))

    send_piece("up", 1)
    send_d(0)
    for r in range(nq):
        turn(0, r)
    send_piece("dn", 0)
    send_piece("dn", 2)
    side("up", 0)
    send_d(1)
    send_d(2)
    send_piece("dn", 1)
    forward("dn", 2, 1)
    forward("dn", 0, 1)
    send_d(3)
    send_x()
    forward("dn", 2, 2)
    d_back(1)
    forward("dn", 0, 2)
    d_back(0)
    side("dn", 2)
    side("dn", 1)
    side("dn", 0)
    send_piece("up", 3)
    forward("dn", 0, 3)
    send_piece("dn", 3)
    forward("dn", 1, 1)
    act_own(0)
    send_piece("up", 2)
    forward("dn", 3, 1)
    d_back(2)
    side("up", 1)
    forward("up", 0, 1)
    d_back(3)
    gain_over_y()
    forward("dn", 2, 3)
    side("up", 3)
    act_far(0)
    have_pre(0)
    turn(1, 0)
    grads(0, 0)
    forward("dn", 1, 2)
    sum_step(0, 0, 0)
    turn(1, 2)
    forward("dn", 3, 2)
    forward("up", 2, 1)
    act_own(2)
    side("dn", 3)
    gain_over_z()
    grads(0, 2)
    sum_step(0, 2, 0)
    forward("up", 0, 2)
    forward("up", 1, 1)
    side("up", 2)
    act_far(2)
    have_pre(2)
    grads(2, 0)
    sum_step(2, 0, 0)
    forward("dn", 1, 3)
    turn(1, 1)
    sum_step(0, 2, 1)
    forward("dn", 3, 3)
    grads(0, 1)
    grads(2, 1)
    sum_step(2, 1, 0)
    sum_step(2, 0, 1)
    forward("up", 2, 2)
    grads(2, 2)
    sum_step(0, 1, 0)
    act_own(1)
    forward("up", 3, 1)
    act_far(1)
    act_own(3)
    have_pre(1)
    forward("up", 0, 3)
    grads(1, 1)
    forward("up", 1, 2)
    sum_step(0, 0, 1)
    sum_step(2, 1, 1)
    gain_relay(1)
    sum_step(1, 1, 0)
    grads(1, 2)
    to_y(2, 2)
    sum_step(0, 1, 1)
    act_far(3)
    grads(1, 0)
    forward("up", 2, 3)
    have_pre(3)
    sum_step(1, 2, 0)
    sum_step(2, 0, 2)
    grads(3, 2)
    grads(3, 1)
    forward("up", 3, 2)
    sum_step(3, 1, 0)
    turn(1, 3)
    grads(0, 3)
    sum_step(3, 2, 0)
    sum_step(1, 0, 0)
    forward("up", 1, 3)
    grads(3, 0)
    sum_step(1, 1, 1)
    grads(3, 3)
    to_y(3, 0)
    grads(1, 3)
    sum_step(2, 2, 0)
    sum_step(1, 2, 1)
    grads(2, 3)
    sum_step(0, 0, 2)
    back_far(2)
    to_y(2, 3)
    gain_relay(2)
    to_y(3, 3)
    sum_step(0, 2, 2)
    back_own(2)
    sum_step(3, 1, 1)
    back_far(0)
    back_far(1)
    sum_step(1, 2, 2)
    sum_step(2, 1, 2)
    sum_step(3, 1, 2)
    sum_step(1, 1, 2)
    sum_step(3, 2, 1)
    to_y(1, 3)
    to_y(0, 3)
    sum_step(1, 0, 1)
    sum_step(2, 3, 0)
    sum_step(3, 0, 0)
    sum_step(2, 2, 1)
    sum_step(3, 3, 0)
    sum_step(3, 2, 2)
    forward("up", 3, 3)
    sum_step(1, 3, 0)
    sum_step(2, 1, 3)
    sum_step(0, 3, 0)
    sum_step(3, 2, 3)
    sum_step(3, 1, 3)
    sum_step(2, 0, 3)
    sum_step(1, 1, 3)
    gain_relay(3)
    back_own(1)
    sum_step(0, 2, 3)
    sum_step(0, 1, 2)
    sum_step(3, 0, 1)
    sum_step(1, 0, 2)
    back_far(3)
    sum_step(2, 3, 1)
    back_own(0)
    sum_step(3, 3, 1)
    sum_step(2, 2, 3)
    sum_step(3, 0, 3)
    sum_step(0, 3, 1)
    sum_step(1, 3, 1)
    sum_step(3, 0, 2)
    back_own(3)
    sum_step(1, 2, 3)
    sum_step(3, 3, 3)
    sum_step(0, 0, 3)
    sum_step(0, 1, 3)
    sum_step(2, 2, 2)
    sum_step(1, 0, 3)
    sum_step(3, 3, 2)
    sum_step(2, 3, 2)
    sum_step(2, 3, 3)
    sum_step(1, 3, 2)
    sum_step(1, 3, 3)
    sum_step(0, 3, 3)
    sum_step(0, 3, 2)
    total = gz[0]
    for k in range(1, nz):
        total = total + gz[k]
    gg_out[...] = total * scaled
    for r in range(nq):
        wire.got(gi_got.at[r], ("gi", r))
        gi_out[:, pl.ds(r * high, high)] = (gi_own[r] + gi_got[r].astype(f32)).astype(bf16)
    stage = lax.rem(z * ny + y, nq)
    for r in range(nq):
        tile = pl.ds(r * high, high)
        for q in range(nq):
            if not first_y(q, r):
                @pl.when(stage == q)
                def _():
                    wire.got(tot_got.at[r], ("total", r))
                    gu_out[tile, :] = (gu_out[tile, :] + tot_got[r].astype(f32)) * scaled
    wire.drain()


def kernel_step(fs, tp, inputs, hidden_pre, norm_input, out_gain, w_up, w_down, cotangent):
    nx = ny = 2
    nz = fs // (nx * ny)
    rows, half = inputs.shape
    blk, cols = w_up.shape[1], w_down.shape[1]
    nq = nz * ny // tp
    ns, high = nz * ny, half // nq
    hid = nq * blk
    f32, bf16 = jnp.float32, jnp.bfloat16
    v = pltpu.VMEM
    scratch = [
        v((rows, half), bf16), v((rows, half), bf16), v((1, half), f32),
        v((rows, 128), f32), v((rows, 128), f32),
        v((nx * rows, 2 * half), bf16),
        v((nx, rows, half), bf16), v((half, nx * rows), bf16),
        v((nx, nq, rows, blk), bf16),
        v((hid, 2 * half), bf16), v((half, ns * blk), bf16), v((nx * rows, ns * blk), bf16),
        v((nq, ns, high, blk), f32),
        v((nq, rows, high), f32), v((nq, rows, high), bf16), v((nq, rows, high), bf16),
        v((2, nq, nz, ny, high, blk), bf16),
        v((nq, nz, high, blk), bf16), v((nq, nz, high, blk), bf16),
        v((nq, high, blk), bf16), v((nq, high, blk), bf16), v((nq, high, blk), f32),
        v((8, half), f32),
        v((1, half), f32), v((1, half), f32), v((1, half), f32), v((1, half), f32),
        v((nz, 1, half), f32),
        pltpu.SemaphoreType.DMA((3 + 3 * nq + 1,)),
        pltpu.SemaphoreType.DMA((SENDS,)), pltpu.SemaphoreType.DMA((RECVS,)),
    ]
    flops = 3 * 2 * nx * rows * 2 * half * hid
    shapes = ((rows, half), bf16), ((half, blk), f32), ((1, half), f32)
    results = pl.pallas_call(
        functools.partial(fused, nz, ny),
        out_shape=tuple(v(*shape) for shape in shapes),
        in_specs=[pl.BlockSpec(memory_space=pl.ANY)] * 7,
        out_specs=(pl.BlockSpec(memory_space=pltpu.VMEM),) * 3,
        scratch_shapes=scratch,
        compiler_params=pltpu.CompilerParams(
            collective_id=0, has_side_effects=True, vmem_limit_bytes=60 << 20
        ),
        cost_estimate=pl.CostEstimate(flops=flops, bytes_accessed=1 << 24, transcendentals=0),
        name="layer_backward",
    )(
        inputs, hidden_pre, norm_input, out_gain.reshape(1, half), w_up,
        w_down.reshape(nq, nx, blk, cols), cotangent,
    )
    grad_input, grad_up, grad_gain = results
    return grad_input, grad_up, grad_gain.reshape(half)


def in_kernel(*args):
    return kernel_step(lax.axis_size("fs"), lax.axis_size("tp"), *args)


def solution(mesh):
    placed = (
        P("fs", "tp"),
        P("fs", "tp"),
        P("fs", "tp"),
        P("tp"),
        P("tp", "fs"),
        P("tp", "fs"),
        P("fs", "tp"),
    )
    fs, tp = mesh.shape["fs"], mesh.shape["tp"]
    out_specs = (P("fs", "tp"), P("tp", "fs"), P("tp"))

    def solve(*args):
        up, down = args[4].shape, args[5].shape
        whole = up[1] // fs % 128 == 0 and down[1] // fs % 128 == 0
        if tp == 2 and fs == 4 * PLAN_STEPS and whole:
            return jax.shard_map(
                in_kernel, mesh=mesh, in_specs=placed, out_specs=out_specs, check_vma=False
            )(*args)
        return permuted(*args)

    step = jax.shard_map(
        on_device,
        mesh=mesh,
        in_specs=placed,
        out_specs=(P("fs", "tp"), P("tp", "fs"), P("tp")),
        check_vma=False,
    )
    permuted = step
    return solve
```

```python
import functools
import math

import jax
import jax.numpy as jnp
from jax import lax
from jax.experimental import pallas as pl
from jax.experimental.pallas import tpu as pltpu
from jax.sharding import PartitionSpec as P


norm_eps = 1e-06
MESH = pl.DeviceIdType.MESH
SENDS = 93
RECVS = 157
PLAN_STEPS = 4
FULL_SIDE = ()
Y_FIRST = ((0, 3), (1, 3), (2, 2), (2, 3), (3, 0), (3, 3))
X_ORDER = (("pre", 0), ("inp", 0), ("inp", 2), ("pre", 2), ("inp", 1), ("pre", 1), ("pre", 3), ("inp", 3))


def trade(x, axis, mask):
    if mask == 0:
        return x
    return lax.ppermute(x, axis, [(i, i ^ mask) for i in range(lax.axis_size(axis))])


def total(x, axis):
    step = 1
    while step < lax.axis_size(axis):
        x = x + trade(x, axis, step)
        step *= 2
    return x


def masks_of(n):
    masks = [1 << i for i in range(n.bit_length() - 1)]
    return (masks, masks[::-1])


def halves(x):
    rows = x.shape[0] // 2
    return (x[:rows], x[rows:])


def gather_near(x, near_n):
    parts = []
    for part, masks in zip(halves(x), masks_of(near_n)):
        held = {0: part}
        for mask in masks:
            held.update({k ^ mask: trade(v, "fs", mask) for k, v in list(held.items())})
        parts.append(held)
    return parts


def scatter_near(pieces, near_n):
    sums = []
    for side, masks in enumerate(masks_of(near_n)):
        held = {k: halves(v)[side] for k, v in pieces.items()}
        for mask in masks:
            sent = {k: held.pop(k) for k in list(held) if k & mask}
            for k, v in sent.items():
                came = trade(v.astype(jnp.bfloat16), "fs", mask).astype(jnp.float32)
                held[k ^ mask] = held[k ^ mask] + came
        sums.append(held[0])
    return jnp.concatenate(sums, axis=0)


def tree(x, n, unit):
    terms = [trade(x, "fs", k * unit) for k in range(n)]
    while len(terms) > 1:
        terms = [a + b for a, b in zip(terms[::2], terms[1::2])]
    return terms[0]


def pick(stack, index):
    return lax.dynamic_index_in_dim(stack, index, 0, keepdims=False)


def dot(a, b, dim):
    return lax.dot_general(
        a, b, (((dim,), (dim,)), ((), ())), preferred_element_type=jnp.float32
    )


def on_device(inputs, hidden_pre, norm_input, out_gain, w_up, w_down, cotangent):
    fs, tp = lax.axis_size("fs"), lax.axis_size("tp")
    near_n = 1
    while 4 * near_n * near_n <= fs:
        near_n *= 2
    far_n = fs // near_n
    per = far_n // tp
    me, core = lax.axis_index("fs"), lax.axis_index("tp")
    far, near = me // near_n, me % near_n
    rows = inputs.shape[0]
    width = inputs.shape[1] * tp
    scaled = (rows * fs) ** (-0.5)
    block = w_up.shape[1]
    cols = w_down.shape[1]

    down_rows = w_down.reshape(per, near_n, block, cols)
    asked = [
        lax.dynamic_index_in_dim(down_rows, near ^ k, 1, keepdims=False).reshape(per * block, cols)
        for k in range(near_n)
    ]
    arrived = [trade(x, "fs", k) for k, x in enumerate(asked)]
    arrived = jnp.stack(arrived)
    down_near = jnp.concatenate([pick(arrived, near ^ i) for i in range(near_n)], axis=1)
    down_far = [trade(down_near, "fs", k * near_n) for k in range(far_n)]
    up_far = [trade(w_up, "fs", k * near_n) for k in range(far_n)]
    up_far = jnp.stack(up_far)
    down_far = jnp.stack(down_far)
    down, up = [], []
    for t in range(tp):
        places = [((core ^ t) * per + j) ^ far for j in range(per)]
        down.append(jnp.concatenate([pick(down_far, i) for i in places], axis=1))
        up.append(jnp.concatenate([pick(up_far, i) for i in places], axis=1))

    asked = [
        jnp.concatenate(
            [
                lax.dynamic_slice_in_dim(
                    hidden_pre, (j * near_n + (near ^ k)) * block, block, axis=1
                )
                for j in range(per)
            ],
            axis=1,
        )
        for k in range(near_n)
    ]
    pre = [trade(x, "fs", k) for k, x in enumerate(asked)]

    normed = norm_input.astype(jnp.float32)
    upstream = cotangent.astype(jnp.float32)
    weighted = upstream * out_gain
    sums = total(
        jnp.stack([jnp.sum(normed * normed, axis=1), jnp.sum(weighted * normed, axis=1)]), "tp"
    )
    inv_rms = lax.rsqrt(sums[0] / width + norm_eps)[:, None]
    cross_mean = (sums[1] / width)[:, None]
    d_out = (weighted * inv_rms - normed * inv_rms * inv_rms * inv_rms * cross_mean).astype(
        jnp.bfloat16
    )
    gain = jnp.sum(upstream * normed * inv_rms, axis=0) * scaled
    gain = tree(gain, near_n, 1)
    grad_gain = tree(gain, far_n, near_n)

    d_outs = gather_near(d_out, near_n)
    tokens = gather_near(inputs, near_n)
    d_pres, partial = [], {}
    for k in range(near_n):
        d_out_k = jnp.concatenate([d_outs[0][k], d_outs[1][k]], axis=0)
        d_out_k = [trade(d_out_k, "tp", t) for t in range(tp)]
        d_act = sum(dot(d_out_k[t], down[t], 1) for t in range(tp))
        d_pre = (d_act * 2.0 * jax.nn.relu(pre[k].astype(jnp.float32))).astype(jnp.bfloat16)
        d_pres.append([trade(d_pre, "tp", t) for t in range(tp)])
        partial[k] = sum(dot(d_pres[k][t], up[t], 1) for t in range(tp))
    grad_input = scatter_near(partial, near_n)

    all_pres = [
        jnp.concatenate([d_pres[k][t] for k in range(near_n)], axis=0) for t in range(tp)
    ]
    all_tokens = jnp.concatenate([side[k] for k in range(near_n) for side in tokens], axis=0)
    sums_up = [dot(x, all_tokens, 0) for x in all_pres]
    sums_up = jnp.concatenate(sums_up, axis=0).reshape(
        far_n, block, inputs.shape[1]
    )
    grad_up = 0.0
    for k in range(far_n):
        goal = far ^ k
        mine = pick(sums_up, (core ^ (goal // per)) * per + goal % per)
        if k:
            mine = trade(mine.astype(jnp.bfloat16), "fs", k * near_n).astype(jnp.float32)
        grad_up = grad_up + mine
    return (grad_input.astype(jnp.bfloat16), (grad_up * scaled).T, grad_gain)


def mm(a, b):
    return lax.dot_general(a, b, (((1,), (1,)), ((), ())), preferred_element_type=jnp.float32)


class Wire:
    def __init__(self, send, recv, other, nz):
        self.send, self.recv, self.other, self.nz = send, recv, other, nz
        self.sent, self.came, self.pending, self.groups = {}, {}, [], {}

    def arrives(self, key):
        *head, way, k = key if isinstance(key, tuple) else (key, None, None)
        if key[0] == "sum":
            kind, r, goal, column = key[1:]
            return "sum", r, goal + 1 - kind, column
        if way == "d":
            return *head, "u", self.nz - k
        if way == "y" and k[0] == "d":
            return *head, "y", ("u", self.nz - k[1])
        return key

    def departs(self, key):
        if key[0] == "sum":
            return "sum", *key[2:]
        if isinstance(key, tuple) and key[-2] == "d":
            return key if key[-1] < self.nz - 1 else (*key[:-2], "u", key[-1])
        return self.arrives(key)

    def at(self, sems, names, key):
        index = names.setdefault(key, len(names))
        assert index < sems.shape[0], "semaphores"
        return sems.at[index]

    def put(self, refs, key, device, live=None, group=None):
        out = self.at(self.send, self.sent, group or self.departs(key))
        arrival = self.at(self.recv, self.came, self.arrives(key))

        def copy():
            source, target = refs()
            return pltpu.make_async_remote_copy(
                src_ref=source, dst_ref=target, send_sem=out, recv_sem=arrival,
                device_id=device, device_id_type=MESH,
            )

        when(live, lambda: copy().start())
        if group is None:
            self.pending.append((copy, live))
        else:
            source = refs()[0]
            size = math.prod(source.shape) * source.dtype.itemsize
            self.groups.setdefault(group, [out, live, 0])[2] += size

    def got(self, ref, key):
        pltpu.make_async_remote_copy(
            src_ref=ref, dst_ref=ref, send_sem=self.send.at[0],
            recv_sem=self.at(self.recv, self.came, self.arrives(key)),
            device_id=self.other, device_id_type=MESH,
        ).wait_recv()

    def drain(self, like):
        for copy, live in self.pending:
            when(live, lambda: copy().wait_send())
        for out, live, size in self.groups.values():
            ref = like.at[pl.ds(0, size // (like.shape[1] * like.dtype.itemsize)), :]
            when(live, lambda: pltpu.make_async_remote_copy(
                src_ref=ref, dst_ref=ref, send_sem=out, recv_sem=self.recv.at[0],
                device_id=self.other, device_id_type=MESH,
            ).wait_send())


def when(live, body):
    if live is None:
        body()
    else:
        pl.when(live)(body)


def both(a, b):
    return a if b is None else b if a is None else jnp.logical_and(a, b)


def fused(nz, ny, inp, pre, nrm, gain, wu, wd, cot, gi_out, gu_out, gg_out,
          nrm_v, cot_v, gain_v, st, st2, d_out, inp_v, inp_t, pre_v, dn, up, dp,
          part, gi_own, gi_send, gi_got, chain, y_send, y_got,
          tot_send, tot_got, acc, gacc, gx, gx2, gy, gy2, gz, loc, send, recv):
    nx, f32, bf16 = 2, jnp.float32, jnp.bfloat16
    rows, half = inp.shape
    nq, _, blk, cols = wd.shape
    ns = nz * ny
    width = 2 * half
    wide = nx * cols
    chunks = 4
    step = rows // chunks
    high = half // nq
    scaled = (rows * nz * ny * nx) ** (-0.5)

    me, core = lax.axis_index("fs"), lax.axis_index("tp")
    x, y, z = me % nx, (me // nx) % ny, me // (nx * ny)
    at_x = (me + 1 - 2 * x, core)
    at_y = (me + nx * (1 - 2 * y), core)
    at_up = (me + nx * ny, core)
    at_down = (me - nx * ny, core)
    at_core = (me, 1 - core)
    wire = Wire(send, recv, at_core, nz)
    low_end, top_end = z > 0, z < nz - 1

    def place(zz, yy):
        return lax.rem(zz * ny + yy + core * nq, ns)

    local = {}

    def load(name, refs):
        index = len(local)
        local[name] = (lambda: pltpu.make_async_copy(*refs(), loc.at[index]))
        local[name]().start()

    def ready(name):
        local[name]().wait()

    load("nrm", lambda: (nrm, nrm_v))
    load("cot", lambda: (cot, cot_v))
    load("gain", lambda: (gain, gain_v))

    def own_dn(q, xx):
        start = place(z, y) * wide + xx * cols
        return dn.at[pl.ds(q * blk, blk), pl.ds(pl.multiple_of(start, cols), cols)]

    for q in range(nq):
        load(("dn", q), lambda q=q: (wd.at[q, x], own_dn(q, x)))
    for q in range(nq):
        load(("up", q), lambda q=q: (
            wu.at[pl.ds(q * high, high), :],
            up.at[pl.ds(q * high, high), pl.ds(pl.multiple_of(place(z, y) * blk, blk), blk)]))
    for q in range(nq):
        load(("pre", q), lambda q=q: (
            pre.at[:, pl.ds(pl.multiple_of((2 * q + x) * blk, blk), blk)], pre_v.at[0, q]))
    load("inp", lambda: (inp, inp_v.at[0]))

    barrier = pltpu.get_barrier_semaphore()
    peers = (
        (at_core, None), (at_x, None), (at_y, None), (at_up, top_end), (at_down, low_end),
    )
    for peer, live in peers:
        when(live, lambda: pl.semaphore_signal(
            barrier, inc=1, device_id=peer, device_id_type=MESH))
    count = 3
    for _, live in peers[3:]:
        count = count + live.astype(jnp.int32)

    ready("nrm")
    ready("cot")
    ready("gain")
    gacc[...] = jnp.zeros_like(gacc)
    tall = 32

    def stats(i, carry):
        r = pl.ds(pl.multiple_of(i * tall, tall), tall)
        n = nrm_v[r, :].astype(f32)
        u = cot_v[r, :].astype(f32) * gain_v[...]
        squares = jnp.sum(n * n, axis=1, keepdims=True)
        cross = jnp.sum(u * n, axis=1, keepdims=True)
        lane = lax.broadcasted_iota(jnp.int32, (tall, st.shape[1]), 1)
        st[r, :] = jnp.where(lane == 0, squares, cross)
        return carry

    lax.fori_loop(0, rows // tall, stats, 0)

    pl.semaphore_wait(barrier, count)

    wire.put(lambda: (st, st2), "stats", at_core)
    for q in range(nq):
        wire.put(lambda q=q: (wd.at[q, 1 - x], own_dn(q, x)), ("swap", q), at_x, None, "swap")


    def piece(name, j, zz, yy, part_of=0):
        buf, tile, w = gathers[name]
        first = (0, 0, tile // 2)[part_of]
        count = (tile, tile // 2, tile // 2)[part_of]
        return buf.at[pl.ds(j * tile + first, count),
                      pl.ds(pl.multiple_of(place(zz, yy) * w, w), w)]

    gathers = {"dn": (dn, blk, wide), "up": (up, high, blk)}
    odd = z % 2 == 1
    even = jnp.logical_not(odd)

    def over_y(name, j, zz, tag, live, halved=None):
        refs = lambda: (piece(name, j, zz, y),) * 2
        half_refs = lambda: (piece(name, j, zz, y, 1),) * 2
        key = (name, j, "y", tag)
        if halved is None:
            wire.put(refs, key, at_y, live, ("y", tag))
        else:
            wire.put(refs, key, at_y, both(live, jnp.logical_not(halved)))
            if (name, j) not in FULL_SIDE:
                wire.put(half_refs, key, at_y, both(live, halved))

    def own(name, j):
        refs = lambda: (piece(name, j, z, y),) * 2
        wire.put(refs, (name, j, "u", 1), at_up, top_end, "own_u")
        wire.put(refs, (name, j, "d", 1), at_down, low_end, "own_d")
        over_y(name, j, z, "own", None)

    def forward(name, j, k):
        for way, zz, live, device, ahead, halved in (
            ("u", z - k, z >= k, at_up, top_end, odd),
            ("d", z + k, z + k < nz, at_down, low_end, even),
        ):
            when(live, lambda: wire.got(piece(name, j, zz, y), (name, j, way, k)))
            if k < nz - 1:
                wire.put(lambda zz=zz: (piece(name, j, zz, y),) * 2, (name, j, way, k + 1),
                         device, both(live, ahead), ("z", way, k))
            over_y(name, j, zz, (way, k), live, halved if k == 1 else None)

    def side(name, j):
        wire.got(piece(name, j, z, 1 - y), (name, j, "y", "own"))
        share = 0 if (name, j) in FULL_SIDE else 2
        refs = lambda: (piece(name, j, z, 1 - y, share),) * 2
        wire.put(refs, (name, j, "side"), at_up, even)
        wire.put(refs, (name, j, "side"), at_down, odd)

    def arrived(name, j):
        for k in range(1, nz):
            for tag, zz, live, halved in (
                ("u", z - k, z >= k, odd), ("d", z + k, z + k < nz, even)
            ):
                key = (name, j, "y", (tag, k))
                if k == 1:
                    if (name, j) not in FULL_SIDE:
                        when(jnp.logical_and(live, halved), lambda: wire.got(
                            piece(name, j, zz, 1 - y, 1), key))
                    live = jnp.logical_and(live, jnp.logical_not(halved))
                when(live, lambda: wire.got(piece(name, j, zz, 1 - y), key))
        share = 0 if (name, j) in FULL_SIDE else 2
        wire.got(piece(name, j, z + 1 - 2 * (z % 2), 1 - y, share), (name, j, "side"))

    def send_piece(name, j):
        ready((name, j))
        if name == "dn":
            wire.got(own_dn(j, 1 - x), ("swap", j))
        own(name, j)

    send_piece("up", 0)

    wire.got(st2, "stats")
    short = 16

    def norm(n_chunk):
        def rows_of(i, carry):
            r = pl.ds(pl.multiple_of(n_chunk * step + i * short, short), short)
            n = nrm_v[r, :].astype(f32)
            u = cot_v[r, :].astype(f32)
            both_sums = st[r, :] + st2[r, :]
            inv = lax.rsqrt(both_sums[:, 0:1] / width + norm_eps)
            cross = both_sums[:, 1:2] / width
            d = u * gain_v[...] * inv - n * (inv * inv * inv * cross)
            d_out[r, pl.ds(0, half)] = d.astype(bf16)
            g = u * n * inv
            gacc[...] += g[0:8] + g[8:16]
            return carry

        lax.fori_loop(0, step // short, rows_of, 0)

    def d_tile(t, n_chunk, h):
        return d_out.at[pl.ds(t * rows + n_chunk * step, step), pl.ds(h * half, half)]

    def send_d(n):
        norm(n)
        wire.put(lambda: (d_tile(0, n, 0), d_tile(1, n, 0)), ("d_x", n), at_x, None, "d_x")
        wire.put(lambda: (d_tile(0, n, 0), d_tile(0, n, 1)), ("d_core", 0, n), at_core, None, "d_core")

    def send_x():
        gx[...] = jnp.sum(gacc[...], axis=0, keepdims=True)
        wire.put(lambda: (gx, gx2), "gain_x", at_x)
        for kind, q in X_ORDER:
            if kind == "inp":
                tile = pl.ds(q * high, high)
                wire.put(lambda tile=tile: (inp.at[:, tile], inp_v.at[1, :, tile]),
                         ("inp", q), at_x, None, "inp")
            else:
                wire.put(lambda q=q: (
                    pre.at[:, pl.ds(pl.multiple_of((2 * q + 1 - x) * blk, blk), blk)],
                    pre_v.at[1, q]), ("pre", q), at_x, None, "pre")

    def turn(t, r):
        tile = pl.ds(r * high, high)
        if t == 0:
            if r == 0:
                ready("inp")
        else:
            wire.got(inp_v.at[1, :, tile], ("inp", r))

        def rows_of(i, carry):
            tokens = pl.ds(pl.multiple_of(i * blk, blk), blk)
            inp_t[tile, pl.ds(pl.multiple_of(t * rows + i * blk, blk), blk)] = (
                inp_v[t, tokens, tile].T)
            return carry

        lax.fori_loop(0, rows // blk, rows_of, 0)

    def act(t, q):
        def rows_of(i, carry):
            r = pl.ds(pl.multiple_of(t * rows + i * blk, blk), blk)
            got = mm(d_out[r, :], dn[pl.ds(q * blk, blk), :])
            p = pre_v[t, q, pl.ds(pl.multiple_of(i * blk, blk), blk), :].astype(f32)
            dp[r, pl.ds(q * blk, blk)] = (got * 2.0 * jnp.maximum(p, 0.0)).astype(bf16)
            return carry

        lax.fori_loop(0, rows // blk, rows_of, 0)
        tile = lambda s: dp.at[pl.ds(t * rows, rows), pl.ds((s * nq + q) * blk, blk)]
        wire.put(lambda: (tile(0), tile(1)), ("dp", t, q), at_core, None, "dp")

    def d_back(n):
        wire.got(d_tile(1, n, 0), ("d_x", n))
        wire.put(lambda: (d_tile(1, n, 0), d_tile(1, n, 1)), ("d_core", 1, n), at_core, None, "d_core")

    def act_own(q):
        if q == 0:
            for n in range(chunks):
                wire.got(d_tile(0, n, 1), ("d_core", 0, n))
        ready(("pre", q))
        arrived("dn", q)
        act(0, q)

    def act_far(q):
        if q == 0:
            for n in range(chunks):
                wire.got(d_tile(1, n, 1), ("d_core", 1, n))
        wire.got(pre_v.at[1, q], ("pre", q))
        act(1, q)

    def back_far(r):
        arrived("up", r)

        def rows_of(i, carry):
            k = pl.ds(pl.multiple_of(i * blk, blk), blk)
            w = up[pl.ds(r * high, high), :]
            far = mm(dp[pl.ds(pl.multiple_of(rows + i * blk, blk), blk), :], w)
            gi_send[r, k, :] = far.astype(bf16)
            return carry

        lax.fori_loop(0, rows // blk, rows_of, 0)
        wire.put(lambda: (gi_send.at[r], gi_got.at[r]), ("gi", r), at_x, None, "gi")

    def back_own(r):
        def rows_of(i, carry):
            k = pl.ds(pl.multiple_of(i * blk, blk), blk)
            w = up[pl.ds(r * high, high), :]
            gi_own[r, k, :] = mm(dp[k, :], w)
            return carry

        lax.fori_loop(0, rows // blk, rows_of, 0)

    def have_pre(q):
        for t in range(nx):
            wire.got(dp.at[pl.ds(t * rows, rows), pl.ds((nq + q) * blk, blk)], ("dp", t, q))

    def grads(q, r):
        for j in (q, nq + q):
            part[r, j] = lax.dot_general(
                inp_t[pl.ds(r * high, high), :], dp[:, pl.ds(j * blk, blk)],
                (((1,), (0,)), ((), ())), preferred_element_type=f32)

    def goals(q):
        return [divmod(b, ny) for b in (q, nq + q)]

    def first_y(q, r):
        return (q, r) in Y_FIRST

    def to_y(q, r):
        if not first_y(q, r):
            return
        for goal, column in goals(q):
            live = y != column

            @pl.when(live)
            def _():
                y_send[r, goal] = part[r, place(goal, column)].astype(bf16)

            wire.put(lambda goal=goal: (y_send.at[r, goal], y_got.at[r, goal]),
                     ("y", r, goal), at_y, live)

    def link(q, r, level):
        for goal, column in goals(q):
            for kind in range(2):
                at = level if kind == 0 else nz - 1 - level
                if at >= goal if kind == 0 else at <= goal:
                    continue
                slot = chain.at[kind, r, goal, column]
                key = ("sum", kind, r, goal, column)
                live = z == at
                if first_y(q, r):
                    live = jnp.logical_and(live, y == column)

                @pl.when(live)
                def _():
                    value = part[r, place(goal, column)]
                    if first_y(q, r):
                        wire.got(y_got.at[r, goal], ("y", r, goal))
                        value = value + y_got[r, goal].astype(f32)
                    if level > 0:
                        wire.got(slot, key)
                        value = value + slot[...].astype(f32)
                    slot[...] = value.astype(bf16)

                wire.put(lambda slot=slot: (slot, slot), key,
                         at_up if kind == 0 else at_down, live)

    def settle(q, r):
        for goal, column in goals(q):
            live = z == goal
            if first_y(q, r):
                live = jnp.logical_and(live, y == column)

            @pl.when(live)
            def _():
                value = part[r, place(goal, column)]
                if first_y(q, r):
                    wire.got(y_got.at[r, goal], ("y", r, goal))
                    value = value + y_got[r, goal].astype(f32)
                for kind in range(2):
                    if goal != (0, nz - 1)[kind]:
                        slot = chain.at[kind, r, goal, column]
                        wire.got(slot, ("sum", kind, r, goal, column))
                        value = value + slot[...].astype(f32)
                if first_y(q, r):
                    gu_out[pl.ds(r * high, high), :] = value * scaled
                else:
                    acc[r] = value

            if not first_y(q, r):
                away = jnp.logical_and(live, y != column)

                @pl.when(away)
                def _():
                    tot_send[r] = acc[r].astype(bf16)

                @pl.when(jnp.logical_and(live, y == column))
                def _():
                    gu_out[pl.ds(r * high, high), :] = acc[r]

                wire.put(lambda: (tot_send.at[r], tot_got.at[r]), ("total", r), at_y, away)

    def sum_step(q, r, level):
        if level < nz - 1:
            link(q, r, level)
        else:
            settle(q, r)

    def gain_over_y():
        wire.got(gx2, "gain_x")
        gy[...] = gx[...] + gx2[...]
        wire.put(lambda: (gy, gy2), "gain_y", at_y)

    def gain_over_z():
        wire.got(gy2, "gain_y")
        gz[z] = gy[...] + gy2[...]
        wire.put(lambda: (gz.at[z], gz.at[z]), ("gain", "u", 1), at_up, top_end)
        wire.put(lambda: (gz.at[z], gz.at[z]), ("gain", "d", 1), at_down, low_end)

    def gain_relay(k):
        for key, slot, live, device, ahead in (
            ("u", z - k, z >= k, at_up, top_end), ("d", z + k, z + k < nz, at_down, low_end)
        ):
            when(live, lambda: wire.got(gz.at[slot], ("gain", key, k)))
            if k + 1 < nz:
                wire.put(lambda slot=slot: (gz.at[slot], gz.at[slot]), ("gain", key, k + 1),
                         device, both(live, ahead))

    send_piece("up", 1)
    send_d(0)
    for r in range(nq):
        turn(0, r)
    send_piece("dn", 0)
    send_piece("dn", 2)
    side("up", 0)
    send_d(1)
    send_d(2)
    send_piece("dn", 1)
    forward("dn", 2, 1)
    forward("dn", 0, 1)
    send_d(3)
    send_x()
    forward("dn", 2, 2)
    d_back(1)
    forward("dn", 0, 2)
    d_back(0)
    side("dn", 2)
    side("dn", 1)
    side("dn", 0)
    send_piece("up", 3)
    forward("dn", 0, 3)
    send_piece("dn", 3)
    forward("dn", 1, 1)
    act_own(0)
    send_piece("up", 2)
    forward("dn", 3, 1)
    d_back(2)
    side("up", 1)
    forward("up", 0, 1)
    d_back(3)
    gain_over_y()
    forward("dn", 2, 3)
    side("up", 3)
    act_far(0)
    have_pre(0)
    turn(1, 0)
    grads(0, 0)
    forward("dn", 1, 2)
    sum_step(0, 0, 0)
    turn(1, 2)
    forward("dn", 3, 2)
    forward("up", 2, 1)
    act_own(2)
    side("dn", 3)
    gain_over_z()
    grads(0, 2)
    sum_step(0, 2, 0)
    forward("up", 0, 2)
    forward("up", 1, 1)
    side("up", 2)
    act_far(2)
    have_pre(2)
    grads(2, 0)
    sum_step(2, 0, 0)
    forward("dn", 1, 3)
    turn(1, 1)
    sum_step(0, 2, 1)
    forward("dn", 3, 3)
    grads(0, 1)
    grads(2, 1)
    sum_step(2, 1, 0)
    sum_step(2, 0, 1)
    forward("up", 2, 2)
    grads(2, 2)
    sum_step(0, 1, 0)
    act_own(1)
    forward("up", 3, 1)
    act_far(1)
    act_own(3)
    have_pre(1)
    forward("up", 0, 3)
    grads(1, 1)
    forward("up", 1, 2)
    sum_step(0, 0, 1)
    sum_step(2, 1, 1)
    gain_relay(1)
    sum_step(1, 1, 0)
    grads(1, 2)
    to_y(2, 2)
    sum_step(0, 1, 1)
    act_far(3)
    grads(1, 0)
    forward("up", 2, 3)
    have_pre(3)
    sum_step(1, 2, 0)
    sum_step(2, 0, 2)
    grads(3, 2)
    grads(3, 1)
    forward("up", 3, 2)
    sum_step(3, 1, 0)
    turn(1, 3)
    grads(0, 3)
    sum_step(3, 2, 0)
    sum_step(1, 0, 0)
    forward("up", 1, 3)
    grads(3, 0)
    sum_step(1, 1, 1)
    grads(3, 3)
    to_y(3, 0)
    grads(1, 3)
    sum_step(2, 2, 0)
    sum_step(1, 2, 1)
    grads(2, 3)
    sum_step(0, 0, 2)
    back_far(2)
    to_y(2, 3)
    gain_relay(2)
    to_y(3, 3)
    sum_step(0, 2, 2)
    back_own(2)
    sum_step(3, 1, 1)
    back_far(0)
    back_far(1)
    sum_step(1, 2, 2)
    sum_step(2, 1, 2)
    sum_step(3, 1, 2)
    sum_step(1, 1, 2)
    sum_step(3, 2, 1)
    to_y(1, 3)
    to_y(0, 3)
    sum_step(1, 0, 1)
    sum_step(2, 3, 0)
    sum_step(3, 0, 0)
    sum_step(2, 2, 1)
    sum_step(3, 3, 0)
    sum_step(3, 2, 2)
    forward("up", 3, 3)
    sum_step(1, 3, 0)
    sum_step(2, 1, 3)
    sum_step(0, 3, 0)
    sum_step(3, 2, 3)
    sum_step(3, 1, 3)
    sum_step(2, 0, 3)
    sum_step(1, 1, 3)
    gain_relay(3)
    back_own(1)
    sum_step(0, 2, 3)
    sum_step(0, 1, 2)
    sum_step(3, 0, 1)
    sum_step(1, 0, 2)
    back_far(3)
    sum_step(2, 3, 1)
    back_own(0)
    sum_step(3, 3, 1)
    sum_step(2, 2, 3)
    sum_step(3, 0, 3)
    sum_step(0, 3, 1)
    sum_step(1, 3, 1)
    sum_step(3, 0, 2)
    back_own(3)
    sum_step(1, 2, 3)
    sum_step(3, 3, 3)
    sum_step(0, 0, 3)
    sum_step(0, 1, 3)
    sum_step(2, 2, 2)
    sum_step(1, 0, 3)
    sum_step(3, 3, 2)
    sum_step(2, 3, 2)
    sum_step(2, 3, 3)
    sum_step(1, 3, 2)
    sum_step(1, 3, 3)
    sum_step(0, 3, 3)
    sum_step(0, 3, 2)
    total = gz[0]
    for k in range(1, nz):
        total = total + gz[k]
    gg_out[...] = total * scaled
    for r in range(nq):
        wire.got(gi_got.at[r], ("gi", r))
        gi_out[:, pl.ds(r * high, high)] = (gi_own[r] + gi_got[r].astype(f32)).astype(bf16)
    stage = lax.rem(z * ny + y, nq)
    for r in range(nq):
        tile = pl.ds(r * high, high)
        for q in range(nq):
            if not first_y(q, r):
                @pl.when(stage == q)
                def _():
                    wire.got(tot_got.at[r], ("total", r))
                    gu_out[tile, :] = (gu_out[tile, :] + tot_got[r].astype(f32)) * scaled
    wire.drain(dn)


def kernel_step(fs, tp, inputs, hidden_pre, norm_input, out_gain, w_up, w_down, cotangent):
    nx = ny = 2
    nz = fs // (nx * ny)
    rows, half = inputs.shape
    blk, cols = w_up.shape[1], w_down.shape[1]
    nq = nz * ny // tp
    ns, high = nz * ny, half // nq
    hid = nq * blk
    f32, bf16 = jnp.float32, jnp.bfloat16
    v = pltpu.VMEM
    scratch = [
        v((rows, half), bf16), v((rows, half), bf16), v((1, half), f32),
        v((rows, 128), f32), v((rows, 128), f32),
        v((nx * rows, 2 * half), bf16),
        v((nx, rows, half), bf16), v((half, nx * rows), bf16),
        v((nx, nq, rows, blk), bf16),
        v((hid, 2 * half), bf16), v((half, ns * blk), bf16), v((nx * rows, ns * blk), bf16),
        v((nq, ns, high, blk), f32),
        v((nq, rows, high), f32), v((nq, rows, high), bf16), v((nq, rows, high), bf16),
        v((2, nq, nz, ny, high, blk), bf16),
        v((nq, nz, high, blk), bf16), v((nq, nz, high, blk), bf16),
        v((nq, high, blk), bf16), v((nq, high, blk), bf16), v((nq, high, blk), f32),
        v((8, half), f32),
        v((1, half), f32), v((1, half), f32), v((1, half), f32), v((1, half), f32),
        v((nz, 1, half), f32),
        pltpu.SemaphoreType.DMA((3 + 3 * nq + 1,)),
        pltpu.SemaphoreType.DMA((SENDS,)), pltpu.SemaphoreType.DMA((RECVS,)),
    ]
    flops = 3 * 2 * nx * rows * 2 * half * hid
    shapes = ((rows, half), bf16), ((half, blk), f32), ((1, half), f32)
    results = pl.pallas_call(
        functools.partial(fused, nz, ny),
        out_shape=tuple(v(*shape) for shape in shapes),
        in_specs=[pl.BlockSpec(memory_space=pl.ANY)] * 7,
        out_specs=(pl.BlockSpec(memory_space=pltpu.VMEM),) * 3,
        scratch_shapes=scratch,
        compiler_params=pltpu.CompilerParams(
            collective_id=0, has_side_effects=True, vmem_limit_bytes=60 << 20
        ),
        cost_estimate=pl.CostEstimate(flops=flops, bytes_accessed=1 << 24, transcendentals=0),
        name="layer_backward",
    )(
        inputs, hidden_pre, norm_input, out_gain.reshape(1, half), w_up,
        w_down.reshape(nq, nx, blk, cols), cotangent,
    )
    results = [pltpu.with_memory_space_constraint(a, pltpu.VMEM) for a in results]
    grad_input, grad_up, grad_gain = pl.pallas_call(
        deliver,
        out_shape=tuple(jax.ShapeDtypeStruct(*shape) for shape in shapes),
        in_specs=[pl.BlockSpec(memory_space=pltpu.VMEM)] * 3,
        out_specs=(pl.BlockSpec(memory_space=pl.ANY),) * 3,
        scratch_shapes=[pltpu.SemaphoreType.DMA((3,))],
        name="deliver",
    )(*results)
    return grad_input, grad_up, grad_gain.reshape(half)


def deliver(*refs):
    *refs, sems = refs
    copies = [
        pltpu.make_async_copy(refs[i], refs[3 + i], sems.at[i]) for i in range(3)
    ]
    for copy in copies:
        copy.start()
    for copy in copies:
        copy.wait()


def in_kernel(*args):
    return kernel_step(lax.axis_size("fs"), lax.axis_size("tp"), *args)


def solution(mesh):
    placed = (
        P("fs", "tp"),
        P("fs", "tp"),
        P("fs", "tp"),
        P("tp"),
        P("tp", "fs"),
        P("tp", "fs"),
        P("fs", "tp"),
    )
    fs, tp = mesh.shape["fs"], mesh.shape["tp"]
    out_specs = (P("fs", "tp"), P("tp", "fs"), P("tp"))

    def solve(*args):
        up, down = args[4].shape, args[5].shape
        whole = up[1] // fs % 128 == 0 and down[1] // fs % 128 == 0
        if tp == 2 and fs == 4 * PLAN_STEPS and whole:
            return jax.shard_map(
                in_kernel, mesh=mesh, in_specs=placed, out_specs=out_specs, check_vma=False
            )(*args)
        return permuted(*args)

    step = jax.shard_map(
        on_device,
        mesh=mesh,
        in_specs=placed,
        out_specs=(P("fs", "tp"), P("tp", "fs"), P("tp")),
        check_vma=False,
    )
    permuted = step
    return solve
```

```python
import functools
import math

import jax
import jax.numpy as jnp
from jax import lax
from jax.experimental import pallas as pl
from jax.experimental.pallas import tpu as pltpu
from jax.sharding import PartitionSpec as P


norm_eps = 1e-06
MESH = pl.DeviceIdType.MESH
SENDS = 99
RECVS = 163
PLAN_STEPS = 4
FULL_SIDE = (("dn", 2),)
Y_FIRST = ((0, 1), (0, 3), (1, 0), (1, 3), (2, 2), (2, 3), (3, 1), (3, 3))
X_ORDER = (("pre", 0), ("pre", 3), ("inp", 2), ("inp", 0), ("pre", 1), ("inp", 1), ("pre", 2), ("inp", 3))


def trade(x, axis, mask):
    if mask == 0:
        return x
    return lax.ppermute(x, axis, [(i, i ^ mask) for i in range(lax.axis_size(axis))])


def total(x, axis):
    step = 1
    while step < lax.axis_size(axis):
        x = x + trade(x, axis, step)
        step *= 2
    return x


def masks_of(n):
    masks = [1 << i for i in range(n.bit_length() - 1)]
    return (masks, masks[::-1])


def halves(x):
    rows = x.shape[0] // 2
    return (x[:rows], x[rows:])


def gather_near(x, near_n):
    parts = []
    for part, masks in zip(halves(x), masks_of(near_n)):
        held = {0: part}
        for mask in masks:
            held.update({k ^ mask: trade(v, "fs", mask) for k, v in list(held.items())})
        parts.append(held)
    return parts


def scatter_near(pieces, near_n):
    sums = []
    for side, masks in enumerate(masks_of(near_n)):
        held = {k: halves(v)[side] for k, v in pieces.items()}
        for mask in masks:
            sent = {k: held.pop(k) for k in list(held) if k & mask}
            for k, v in sent.items():
                came = trade(v.astype(jnp.bfloat16), "fs", mask).astype(jnp.float32)
                held[k ^ mask] = held[k ^ mask] + came
        sums.append(held[0])
    return jnp.concatenate(sums, axis=0)


def tree(x, n, unit):
    terms = [trade(x, "fs", k * unit) for k in range(n)]
    while len(terms) > 1:
        terms = [a + b for a, b in zip(terms[::2], terms[1::2])]
    return terms[0]


def pick(stack, index):
    return lax.dynamic_index_in_dim(stack, index, 0, keepdims=False)


def dot(a, b, dim):
    return lax.dot_general(
        a, b, (((dim,), (dim,)), ((), ())), preferred_element_type=jnp.float32
    )


def on_device(inputs, hidden_pre, norm_input, out_gain, w_up, w_down, cotangent):
    fs, tp = lax.axis_size("fs"), lax.axis_size("tp")
    near_n = 1
    while 4 * near_n * near_n <= fs:
        near_n *= 2
    far_n = fs // near_n
    per = far_n // tp
    me, core = lax.axis_index("fs"), lax.axis_index("tp")
    far, near = me // near_n, me % near_n
    rows = inputs.shape[0]
    width = inputs.shape[1] * tp
    scaled = (rows * fs) ** (-0.5)
    block = w_up.shape[1]
    cols = w_down.shape[1]

    down_rows = w_down.reshape(per, near_n, block, cols)
    asked = [
        lax.dynamic_index_in_dim(down_rows, near ^ k, 1, keepdims=False).reshape(per * block, cols)
        for k in range(near_n)
    ]
    arrived = [trade(x, "fs", k) for k, x in enumerate(asked)]
    arrived = jnp.stack(arrived)
    down_near = jnp.concatenate([pick(arrived, near ^ i) for i in range(near_n)], axis=1)
    down_far = [trade(down_near, "fs", k * near_n) for k in range(far_n)]
    up_far = [trade(w_up, "fs", k * near_n) for k in range(far_n)]
    up_far = jnp.stack(up_far)
    down_far = jnp.stack(down_far)
    down, up = [], []
    for t in range(tp):
        places = [((core ^ t) * per + j) ^ far for j in range(per)]
        down.append(jnp.concatenate([pick(down_far, i) for i in places], axis=1))
        up.append(jnp.concatenate([pick(up_far, i) for i in places], axis=1))

    asked = [
        jnp.concatenate(
            [
                lax.dynamic_slice_in_dim(
                    hidden_pre, (j * near_n + (near ^ k)) * block, block, axis=1
                )
                for j in range(per)
            ],
            axis=1,
        )
        for k in range(near_n)
    ]
    pre = [trade(x, "fs", k) for k, x in enumerate(asked)]

    normed = norm_input.astype(jnp.float32)
    upstream = cotangent.astype(jnp.float32)
    weighted = upstream * out_gain
    sums = total(
        jnp.stack([jnp.sum(normed * normed, axis=1), jnp.sum(weighted * normed, axis=1)]), "tp"
    )
    inv_rms = lax.rsqrt(sums[0] / width + norm_eps)[:, None]
    cross_mean = (sums[1] / width)[:, None]
    d_out = (weighted * inv_rms - normed * inv_rms * inv_rms * inv_rms * cross_mean).astype(
        jnp.bfloat16
    )
    gain = jnp.sum(upstream * normed * inv_rms, axis=0) * scaled
    gain = tree(gain, near_n, 1)
    grad_gain = tree(gain, far_n, near_n)

    d_outs = gather_near(d_out, near_n)
    tokens = gather_near(inputs, near_n)
    d_pres, partial = [], {}
    for k in range(near_n):
        d_out_k = jnp.concatenate([d_outs[0][k], d_outs[1][k]], axis=0)
        d_out_k = [trade(d_out_k, "tp", t) for t in range(tp)]
        d_act = sum(dot(d_out_k[t], down[t], 1) for t in range(tp))
        d_pre = (d_act * 2.0 * jax.nn.relu(pre[k].astype(jnp.float32))).astype(jnp.bfloat16)
        d_pres.append([trade(d_pre, "tp", t) for t in range(tp)])
        partial[k] = sum(dot(d_pres[k][t], up[t], 1) for t in range(tp))
    grad_input = scatter_near(partial, near_n)

    all_pres = [
        jnp.concatenate([d_pres[k][t] for k in range(near_n)], axis=0) for t in range(tp)
    ]
    all_tokens = jnp.concatenate([side[k] for k in range(near_n) for side in tokens], axis=0)
    sums_up = [dot(x, all_tokens, 0) for x in all_pres]
    sums_up = jnp.concatenate(sums_up, axis=0).reshape(
        far_n, block, inputs.shape[1]
    )
    grad_up = 0.0
    for k in range(far_n):
        goal = far ^ k
        mine = pick(sums_up, (core ^ (goal // per)) * per + goal % per)
        if k:
            mine = trade(mine.astype(jnp.bfloat16), "fs", k * near_n).astype(jnp.float32)
        grad_up = grad_up + mine
    return (grad_input.astype(jnp.bfloat16), (grad_up * scaled).T, grad_gain)


def mm(a, b):
    return lax.dot_general(a, b, (((1,), (1,)), ((), ())), preferred_element_type=jnp.float32)


class Wire:
    def __init__(self, send, recv, other, nz):
        self.send, self.recv, self.other, self.nz = send, recv, other, nz
        self.sent, self.came, self.pending, self.groups = {}, {}, [], {}

    def arrives(self, key):
        *head, way, k = key if isinstance(key, tuple) else (key, None, None)
        if key[0] == "sum":
            kind, r, goal, column = key[1:]
            return "sum", r, goal + 1 - kind, column
        if way == "d":
            return *head, "u", self.nz - k
        if way == "y" and k[0] == "d":
            return *head, "y", ("u", self.nz - k[1])
        return key

    def departs(self, key):
        if key[0] == "sum":
            return "sum", *key[2:]
        if isinstance(key, tuple) and key[-2] == "d":
            return key if key[-1] < self.nz - 1 else (*key[:-2], "u", key[-1])
        return self.arrives(key)

    def at(self, sems, names, key):
        index = names.setdefault(key, len(names))
        assert index < sems.shape[0], "semaphores"
        return sems.at[index]

    def put(self, refs, key, device, live=None, group=None):
        out = self.at(self.send, self.sent, group or self.departs(key))
        arrival = self.at(self.recv, self.came, self.arrives(key))

        def copy():
            source, target = refs()
            return pltpu.make_async_remote_copy(
                src_ref=source, dst_ref=target, send_sem=out, recv_sem=arrival,
                device_id=device, device_id_type=MESH,
            )

        when(live, lambda: copy().start())
        if group is None:
            self.pending.append((copy, live))
        else:
            source = refs()[0]
            size = math.prod(source.shape) * source.dtype.itemsize
            self.groups.setdefault(group, [out, live, 0])[2] += size

    def got(self, ref, key):
        pltpu.make_async_remote_copy(
            src_ref=ref, dst_ref=ref, send_sem=self.send.at[0],
            recv_sem=self.at(self.recv, self.came, self.arrives(key)),
            device_id=self.other, device_id_type=MESH,
        ).wait_recv()

    def drain(self, like):
        for copy, live in self.pending:
            when(live, lambda: copy().wait_send())
        for out, live, size in self.groups.values():
            ref = like.at[pl.ds(0, size // (like.shape[1] * like.dtype.itemsize)), :]
            when(live, lambda: pltpu.make_async_remote_copy(
                src_ref=ref, dst_ref=ref, send_sem=out, recv_sem=self.recv.at[0],
                device_id=self.other, device_id_type=MESH,
            ).wait_send())


def when(live, body):
    if live is None:
        body()
    else:
        pl.when(live)(body)


def both(a, b):
    return a if b is None else b if a is None else jnp.logical_and(a, b)


def fused(nz, ny, inp, pre, nrm, gain, wu, wd, cot, gi_out, gu_out, gg_out,
          nrm_v, cot_v, gain_v, st, st2, d_out, inp_v, inp_t, pre_v, dn, up, dp,
          part, gi_own, gi_send, gi_got, chain, y_send, y_got,
          tot_send, tot_got, acc, gacc, gx, gx2, gy, gy2, gz, loc, send, recv):
    nx, f32, bf16 = 2, jnp.float32, jnp.bfloat16
    rows, half = inp.shape
    nq, _, blk, cols = wd.shape
    ns = nz * ny
    width = 2 * half
    wide = nx * cols
    chunks = 4
    step = rows // chunks
    high = half // nq
    scaled = (rows * nz * ny * nx) ** (-0.5)

    me, core = lax.axis_index("fs"), lax.axis_index("tp")
    x, y, z = me % nx, (me // nx) % ny, me // (nx * ny)
    at_x = (me + 1 - 2 * x, core)
    at_y = (me + nx * (1 - 2 * y), core)
    at_up = (me + nx * ny, core)
    at_down = (me - nx * ny, core)
    at_core = (me, 1 - core)
    wire = Wire(send, recv, at_core, nz)
    low_end, top_end = z > 0, z < nz - 1

    def place(zz, yy):
        return lax.rem(zz * ny + yy + core * nq, ns)

    local = {}

    def load(name, refs):
        index = len(local)
        local[name] = (lambda: pltpu.make_async_copy(*refs(), loc.at[index]))
        local[name]().start()

    def ready(name):
        local[name]().wait()

    load("nrm", lambda: (nrm, nrm_v))
    load("cot", lambda: (cot, cot_v))
    load("gain", lambda: (gain, gain_v))

    def own_dn(q, xx):
        start = place(z, y) * wide + xx * cols
        return dn.at[pl.ds(q * blk, blk), pl.ds(pl.multiple_of(start, cols), cols)]

    for q in range(nq):
        load(("dn", q), lambda q=q: (wd.at[q, x], own_dn(q, x)))
    for q in range(nq):
        load(("up", q), lambda q=q: (
            wu.at[pl.ds(q * high, high), :],
            up.at[pl.ds(q * high, high), pl.ds(pl.multiple_of(place(z, y) * blk, blk), blk)]))
    for q in range(nq):
        load(("pre", q), lambda q=q: (
            pre.at[:, pl.ds(pl.multiple_of((2 * q + x) * blk, blk), blk)], pre_v.at[0, q]))
    load("inp", lambda: (inp, inp_v.at[0]))

    barrier = pltpu.get_barrier_semaphore()
    peers = (
        (at_core, None), (at_x, None), (at_y, None), (at_up, top_end), (at_down, low_end),
    )
    for peer, live in peers:
        when(live, lambda: pl.semaphore_signal(
            barrier, inc=1, device_id=peer, device_id_type=MESH))
    count = 3
    for _, live in peers[3:]:
        count = count + live.astype(jnp.int32)

    ready("nrm")
    ready("cot")
    ready("gain")
    gacc[...] = jnp.zeros_like(gacc)
    tall = 32

    def stats(i, carry):
        r = pl.ds(pl.multiple_of(i * tall, tall), tall)
        n = nrm_v[r, :].astype(f32)
        u = cot_v[r, :].astype(f32) * gain_v[...]
        squares = jnp.sum(n * n, axis=1, keepdims=True)
        cross = jnp.sum(u * n, axis=1, keepdims=True)
        lane = lax.broadcasted_iota(jnp.int32, (tall, st.shape[1]), 1)
        st[r, :] = jnp.where(lane == 0, squares, cross)
        return carry

    lax.fori_loop(0, rows // tall, stats, 0)

    pl.semaphore_wait(barrier, count)

    wire.put(lambda: (st, st2), "stats", at_core)
    for q in range(nq):
        wire.put(lambda q=q: (wd.at[q, 1 - x], own_dn(q, x)), ("swap", q), at_x, None, "swap")


    def piece(name, j, zz, yy, part_of=0):
        buf, tile, w = gathers[name]
        first = (0, 0, tile // 2)[part_of]
        count = (tile, tile // 2, tile // 2)[part_of]
        return buf.at[pl.ds(j * tile + first, count),
                      pl.ds(pl.multiple_of(place(zz, yy) * w, w), w)]

    gathers = {"dn": (dn, blk, wide), "up": (up, high, blk)}
    odd = z % 2 == 1
    even = jnp.logical_not(odd)

    def over_y(name, j, zz, tag, live, halved=None):
        refs = lambda: (piece(name, j, zz, y),) * 2
        half_refs = lambda: (piece(name, j, zz, y, 1),) * 2
        key = (name, j, "y", tag)
        if halved is None:
            wire.put(refs, key, at_y, live, ("y", tag))
        else:
            wire.put(refs, key, at_y, both(live, jnp.logical_not(halved)))
            if (name, j) not in FULL_SIDE:
                wire.put(half_refs, key, at_y, both(live, halved))

    def own(name, j):
        refs = lambda: (piece(name, j, z, y),) * 2
        wire.put(refs, (name, j, "u", 1), at_up, top_end, "own_u")
        wire.put(refs, (name, j, "d", 1), at_down, low_end, "own_d")
        over_y(name, j, z, "own", None)

    def forward(name, j, k):
        for way, zz, live, device, ahead, halved in (
            ("u", z - k, z >= k, at_up, top_end, odd),
            ("d", z + k, z + k < nz, at_down, low_end, even),
        ):
            when(live, lambda: wire.got(piece(name, j, zz, y), (name, j, way, k)))
            if k < nz - 1:
                wire.put(lambda zz=zz: (piece(name, j, zz, y),) * 2, (name, j, way, k + 1),
                         device, both(live, ahead), ("z", way, k))
            over_y(name, j, zz, (way, k), live, halved if k == 1 else None)

    def side(name, j):
        wire.got(piece(name, j, z, 1 - y), (name, j, "y", "own"))
        share = 0 if (name, j) in FULL_SIDE else 2
        refs = lambda: (piece(name, j, z, 1 - y, share),) * 2
        wire.put(refs, (name, j, "side"), at_up, even)
        wire.put(refs, (name, j, "side"), at_down, odd)

    def arrived(name, j):
        for k in range(1, nz):
            for tag, zz, live, halved in (
                ("u", z - k, z >= k, odd), ("d", z + k, z + k < nz, even)
            ):
                key = (name, j, "y", (tag, k))
                if k == 1:
                    if (name, j) not in FULL_SIDE:
                        when(jnp.logical_and(live, halved), lambda: wire.got(
                            piece(name, j, zz, 1 - y, 1), key))
                    live = jnp.logical_and(live, jnp.logical_not(halved))
                when(live, lambda: wire.got(piece(name, j, zz, 1 - y), key))
        share = 0 if (name, j) in FULL_SIDE else 2
        wire.got(piece(name, j, z + 1 - 2 * (z % 2), 1 - y, share), (name, j, "side"))

    def send_piece(name, j):
        ready((name, j))
        if name == "dn":
            wire.got(own_dn(j, 1 - x), ("swap", j))
        own(name, j)

    send_piece("up", 0)

    wire.got(st2, "stats")
    short = 16

    def norm(n_chunk):
        def rows_of(i, carry):
            r = pl.ds(pl.multiple_of(n_chunk * step + i * short, short), short)
            n = nrm_v[r, :].astype(f32)
            u = cot_v[r, :].astype(f32)
            both_sums = st[r, :] + st2[r, :]
            inv = lax.rsqrt(both_sums[:, 0:1] / width + norm_eps)
            cross = both_sums[:, 1:2] / width
            d = u * gain_v[...] * inv - n * (inv * inv * inv * cross)
            d_out[r, pl.ds(0, half)] = d.astype(bf16)
            g = u * n * inv
            gacc[...] += g[0:8] + g[8:16]
            return carry

        lax.fori_loop(0, step // short, rows_of, 0)

    def d_tile(t, n_chunk, h):
        return d_out.at[pl.ds(t * rows + n_chunk * step, step), pl.ds(h * half, half)]

    def send_d(n):
        norm(n)
        wire.put(lambda: (d_tile(0, n, 0), d_tile(1, n, 0)), ("d_x", n), at_x, None, "d_x")
        wire.put(lambda: (d_tile(0, n, 0), d_tile(0, n, 1)), ("d_core", 0, n), at_core, None, "d_core")

    def send_x():
        gx[...] = jnp.sum(gacc[...], axis=0, keepdims=True)
        wire.put(lambda: (gx, gx2), "gain_x", at_x)
        for kind, q in X_ORDER:
            if kind == "inp":
                tile = pl.ds(q * high, high)
                wire.put(lambda tile=tile: (inp.at[:, tile], inp_v.at[1, :, tile]),
                         ("inp", q), at_x, None, "inp")
            else:
                wire.put(lambda q=q: (
                    pre.at[:, pl.ds(pl.multiple_of((2 * q + 1 - x) * blk, blk), blk)],
                    pre_v.at[1, q]), ("pre", q), at_x, None, "pre")

    def turn(t, r):
        tile = pl.ds(r * high, high)
        if t == 0:
            if r == 0:
                ready("inp")
        else:
            wire.got(inp_v.at[1, :, tile], ("inp", r))

        def rows_of(i, carry):
            tokens = pl.ds(pl.multiple_of(i * blk, blk), blk)
            inp_t[tile, pl.ds(pl.multiple_of(t * rows + i * blk, blk), blk)] = (
                inp_v[t, tokens, tile].T)
            return carry

        lax.fori_loop(0, rows // blk, rows_of, 0)

    def act(t, q):
        def rows_of(i, carry):
            r = pl.ds(pl.multiple_of(t * rows + i * blk, blk), blk)
            got = mm(d_out[r, :], dn[pl.ds(q * blk, blk), :])
            p = pre_v[t, q, pl.ds(pl.multiple_of(i * blk, blk), blk), :].astype(f32)
            dp[r, pl.ds(q * blk, blk)] = (got * 2.0 * jnp.maximum(p, 0.0)).astype(bf16)
            return carry

        lax.fori_loop(0, rows // blk, rows_of, 0)
        tile = lambda s: dp.at[pl.ds(t * rows, rows), pl.ds((s * nq + q) * blk, blk)]
        wire.put(lambda: (tile(0), tile(1)), ("dp", t, q), at_core, None, "dp")

    def d_back(n):
        wire.got(d_tile(1, n, 0), ("d_x", n))
        wire.put(lambda: (d_tile(1, n, 0), d_tile(1, n, 1)), ("d_core", 1, n), at_core, None, "d_core")

    def act_own(q):
        if q == 0:
            for n in range(chunks):
                wire.got(d_tile(0, n, 1), ("d_core", 0, n))
        ready(("pre", q))
        arrived("dn", q)
        act(0, q)

    def act_far(q):
        if q == 0:
            for n in range(chunks):
                wire.got(d_tile(1, n, 1), ("d_core", 1, n))
        wire.got(pre_v.at[1, q], ("pre", q))
        act(1, q)

    def back_far(r):
        arrived("up", r)

        def rows_of(i, carry):
            k = pl.ds(pl.multiple_of(i * blk, blk), blk)
            w = up[pl.ds(r * high, high), :]
            far = mm(dp[pl.ds(pl.multiple_of(rows + i * blk, blk), blk), :], w)
            gi_send[r, k, :] = far.astype(bf16)
            return carry

        lax.fori_loop(0, rows // blk, rows_of, 0)
        wire.put(lambda: (gi_send.at[r], gi_got.at[r]), ("gi", r), at_x, None, "gi")

    def back_own(r):
        def rows_of(i, carry):
            k = pl.ds(pl.multiple_of(i * blk, blk), blk)
            w = up[pl.ds(r * high, high), :]
            gi_own[r, k, :] = mm(dp[k, :], w)
            return carry

        lax.fori_loop(0, rows // blk, rows_of, 0)

    def have_pre(q):
        for t in range(nx):
            wire.got(dp.at[pl.ds(t * rows, rows), pl.ds((nq + q) * blk, blk)], ("dp", t, q))

    def grads(q, r):
        for j in (q, nq + q):
            part[r, j] = lax.dot_general(
                inp_t[pl.ds(r * high, high), :], dp[:, pl.ds(j * blk, blk)],
                (((1,), (0,)), ((), ())), preferred_element_type=f32)

    def goals(q):
        return [divmod(b, ny) for b in (q, nq + q)]

    def first_y(q, r):
        return (q, r) in Y_FIRST

    def to_y(q, r):
        if not first_y(q, r):
            return
        for goal, column in goals(q):
            live = y != column

            @pl.when(live)
            def _():
                y_send[r, goal] = part[r, place(goal, column)].astype(bf16)

            wire.put(lambda goal=goal: (y_send.at[r, goal], y_got.at[r, goal]),
                     ("y", r, goal), at_y, live)

    def link(q, r, level):
        for goal, column in goals(q):
            for kind in range(2):
                at = level if kind == 0 else nz - 1 - level
                if at >= goal if kind == 0 else at <= goal:
                    continue
                slot = chain.at[kind, r, goal, column]
                key = ("sum", kind, r, goal, column)
                live = z == at
                if first_y(q, r):
                    live = jnp.logical_and(live, y == column)

                @pl.when(live)
                def _():
                    value = part[r, place(goal, column)]
                    if first_y(q, r):
                        wire.got(y_got.at[r, goal], ("y", r, goal))
                        value = value + y_got[r, goal].astype(f32)
                    if level > 0:
                        wire.got(slot, key)
                        value = value + slot[...].astype(f32)
                    slot[...] = value.astype(bf16)

                wire.put(lambda slot=slot: (slot, slot), key,
                         at_up if kind == 0 else at_down, live)

    def settle(q, r):
        for goal, column in goals(q):
            live = z == goal
            if first_y(q, r):
                live = jnp.logical_and(live, y == column)

            @pl.when(live)
            def _():
                value = part[r, place(goal, column)]
                if first_y(q, r):
                    wire.got(y_got.at[r, goal], ("y", r, goal))
                    value = value + y_got[r, goal].astype(f32)
                for kind in range(2):
                    if goal != (0, nz - 1)[kind]:
                        slot = chain.at[kind, r, goal, column]
                        wire.got(slot, ("sum", kind, r, goal, column))
                        value = value + slot[...].astype(f32)
                if first_y(q, r):
                    gu_out[pl.ds(r * high, high), :] = value * scaled
                else:
                    acc[r] = value

            if not first_y(q, r):
                away = jnp.logical_and(live, y != column)

                @pl.when(away)
                def _():
                    tot_send[r] = acc[r].astype(bf16)

                @pl.when(jnp.logical_and(live, y == column))
                def _():
                    gu_out[pl.ds(r * high, high), :] = acc[r]

                wire.put(lambda: (tot_send.at[r], tot_got.at[r]), ("total", r), at_y, away)

    def sum_step(q, r, level):
        if level < nz - 1:
            link(q, r, level)
        else:
            settle(q, r)

    def gain_over_y():
        wire.got(gx2, "gain_x")
        gy[...] = gx[...] + gx2[...]
        wire.put(lambda: (gy, gy2), "gain_y", at_y)

    def gain_over_z():
        wire.got(gy2, "gain_y")
        gz[z] = gy[...] + gy2[...]
        wire.put(lambda: (gz.at[z], gz.at[z]), ("gain", "u", 1), at_up, top_end)
        wire.put(lambda: (gz.at[z], gz.at[z]), ("gain", "d", 1), at_down, low_end)

    def gain_relay(k):
        for key, slot, live, device, ahead in (
            ("u", z - k, z >= k, at_up, top_end), ("d", z + k, z + k < nz, at_down, low_end)
        ):
            when(live, lambda: wire.got(gz.at[slot], ("gain", key, k)))
            if k + 1 < nz:
                wire.put(lambda slot=slot: (gz.at[slot], gz.at[slot]), ("gain", key, k + 1),
                         device, both(live, ahead))

    for r in range(nq):
        turn(0, r)
    send_d(0)
    send_piece("up", 1)
    send_piece("dn", 0)
    send_piece("up", 2)
    send_piece("dn", 3)
    send_d(1)
    send_d(2)
    send_piece("dn", 1)
    send_d(3)
    forward("dn", 0, 1)
    send_x()
    forward("dn", 3, 1)
    forward("dn", 1, 1)
    side("dn", 0)
    forward("dn", 0, 2)
    forward("dn", 3, 2)
    send_piece("dn", 2)
    d_back(0)
    forward("up", 0, 1)
    forward("dn", 0, 3)
    forward("dn", 3, 3)
    side("dn", 3)
    forward("dn", 2, 1)
    forward("dn", 1, 2)
    send_piece("up", 3)
    forward("up", 0, 2)
    forward("up", 2, 1)
    d_back(2)
    side("dn", 1)
    act_own(0)
    d_back(1)
    side("up", 2)
    act_own(3)
    d_back(3)
    gain_over_y()
    forward("dn", 2, 2)
    forward("up", 1, 1)
    side("up", 1)
    act_far(0)
    side("dn", 2)
    act_far(3)
    forward("dn", 1, 3)
    turn(1, 2)
    have_pre(3)
    grads(3, 2)
    side("up", 0)
    sum_step(3, 2, 0)
    forward("up", 3, 1)
    gain_over_z()
    have_pre(0)
    turn(1, 0)
    grads(0, 0)
    sum_step(3, 2, 1)
    forward("up", 0, 3)
    sum_step(0, 0, 0)
    grads(3, 0)
    grads(0, 2)
    forward("up", 2, 2)
    act_own(1)
    sum_step(3, 0, 0)
    sum_step(0, 2, 0)
    sum_step(3, 2, 2)
    forward("dn", 2, 3)
    sum_step(0, 0, 1)
    act_far(1)
    have_pre(1)
    forward("up", 1, 2)
    turn(1, 1)
    grads(1, 2)
    side("up", 3)
    grads(1, 0)
    sum_step(3, 0, 1)
    grads(3, 1)
    grads(0, 1)
    to_y(0, 1)
    to_y(1, 0)
    grads(1, 1)
    gain_relay(1)
    sum_step(1, 2, 0)
    act_own(2)
    sum_step(0, 2, 1)
    sum_step(1, 1, 0)
    act_far(2)
    forward("up", 3, 2)
    sum_step(3, 0, 2)
    have_pre(2)
    grads(2, 1)
    grads(2, 0)
    sum_step(2, 0, 0)
    forward("up", 2, 3)
    turn(1, 3)
    grads(2, 2)
    grads(0, 3)
    grads(1, 3)
    grads(3, 3)
    to_y(3, 3)
    sum_step(1, 1, 1)
    sum_step(2, 1, 0)
    sum_step(0, 1, 0)
    grads(2, 3)
    sum_step(0, 0, 2)
    to_y(1, 3)
    to_y(2, 2)
    to_y(2, 3)
    sum_step(3, 3, 0)
    sum_step(1, 2, 1)
    gain_relay(2)
    to_y(3, 1)
    sum_step(2, 0, 1)
    forward("up", 1, 3)
    to_y(0, 3)
    back_far(2)
    back_far(0)
    forward("up", 3, 3)
    sum_step(1, 2, 2)
    back_own(0)
    sum_step(2, 1, 1)
    sum_step(1, 3, 0)
    sum_step(2, 2, 0)
    sum_step(3, 2, 3)
    sum_step(3, 1, 0)
    sum_step(1, 0, 0)
    back_own(2)
    sum_step(0, 1, 1)
    sum_step(0, 0, 3)
    sum_step(2, 3, 0)
    sum_step(2, 0, 2)
    sum_step(3, 0, 3)
    back_far(1)
    sum_step(1, 1, 2)
    sum_step(1, 2, 3)
    sum_step(1, 3, 1)
    sum_step(2, 2, 1)
    gain_relay(3)
    sum_step(0, 3, 0)
    back_far(3)
    sum_step(0, 1, 2)
    sum_step(3, 3, 1)
    sum_step(2, 1, 2)
    sum_step(2, 3, 1)
    back_own(1)
    sum_step(0, 2, 2)
    sum_step(1, 1, 3)
    sum_step(2, 2, 3)
    sum_step(2, 1, 3)
    back_own(3)
    sum_step(2, 2, 2)
    sum_step(3, 1, 1)
    sum_step(2, 0, 3)
    sum_step(0, 3, 1)
    sum_step(3, 3, 3)
    sum_step(1, 3, 2)
    sum_step(2, 3, 3)
    sum_step(0, 2, 3)
    sum_step(1, 0, 1)
    sum_step(2, 3, 2)
    sum_step(1, 0, 2)
    sum_step(3, 3, 2)
    sum_step(3, 1, 2)
    sum_step(0, 3, 2)
    sum_step(0, 1, 3)
    sum_step(1, 3, 3)
    sum_step(3, 1, 3)
    sum_step(0, 3, 3)
    sum_step(1, 0, 3)
    total = gz[0]
    for k in range(1, nz):
        total = total + gz[k]
    gg_out[...] = total * scaled
    for r in range(nq):
        wire.got(gi_got.at[r], ("gi", r))
        gi_out[:, pl.ds(r * high, high)] = (gi_own[r] + gi_got[r].astype(f32)).astype(bf16)
    stage = lax.rem(z * ny + y, nq)
    for r in range(nq):
        tile = pl.ds(r * high, high)
        for q in range(nq):
            if not first_y(q, r):
                @pl.when(stage == q)
                def _():
                    wire.got(tot_got.at[r], ("total", r))
                    gu_out[tile, :] = (gu_out[tile, :] + tot_got[r].astype(f32)) * scaled
    wire.drain(dn)


def kernel_step(fs, tp, inputs, hidden_pre, norm_input, out_gain, w_up, w_down, cotangent):
    nx = ny = 2
    nz = fs // (nx * ny)
    rows, half = inputs.shape
    blk, cols = w_up.shape[1], w_down.shape[1]
    nq = nz * ny // tp
    ns, high = nz * ny, half // nq
    hid = nq * blk
    f32, bf16 = jnp.float32, jnp.bfloat16
    v = pltpu.VMEM
    scratch = [
        v((rows, half), bf16), v((rows, half), bf16), v((1, half), f32),
        v((rows, 128), f32), v((rows, 128), f32),
        v((nx * rows, 2 * half), bf16),
        v((nx, rows, half), bf16), v((half, nx * rows), bf16),
        v((nx, nq, rows, blk), bf16),
        v((hid, 2 * half), bf16), v((half, ns * blk), bf16), v((nx * rows, ns * blk), bf16),
        v((nq, ns, high, blk), f32),
        v((nq, rows, high), f32), v((nq, rows, high), bf16), v((nq, rows, high), bf16),
        v((2, nq, nz, ny, high, blk), bf16),
        v((nq, nz, high, blk), bf16), v((nq, nz, high, blk), bf16),
        v((nq, high, blk), bf16), v((nq, high, blk), bf16), v((nq, high, blk), f32),
        v((8, half), f32),
        v((1, half), f32), v((1, half), f32), v((1, half), f32), v((1, half), f32),
        v((nz, 1, half), f32),
        pltpu.SemaphoreType.DMA((3 + 3 * nq + 1,)),
        pltpu.SemaphoreType.DMA((SENDS,)), pltpu.SemaphoreType.DMA((RECVS,)),
    ]
    flops = 3 * 2 * nx * rows * 2 * half * hid
    shapes = ((rows, half), bf16), ((half, blk), f32), ((1, half), f32)
    results = pl.pallas_call(
        functools.partial(fused, nz, ny),
        out_shape=tuple(v(*shape) for shape in shapes),
        in_specs=[pl.BlockSpec(memory_space=pl.ANY)] * 7,
        out_specs=(pl.BlockSpec(memory_space=pltpu.VMEM),) * 3,
        scratch_shapes=scratch,
        compiler_params=pltpu.CompilerParams(
            collective_id=0, has_side_effects=True, vmem_limit_bytes=60 << 20
        ),
        cost_estimate=pl.CostEstimate(flops=flops, bytes_accessed=1 << 24, transcendentals=0),
        name="layer_backward",
    )(
        inputs, hidden_pre, norm_input, out_gain.reshape(1, half), w_up,
        w_down.reshape(nq, nx, blk, cols), cotangent,
    )
    results = [pltpu.with_memory_space_constraint(a, pltpu.VMEM) for a in results]
    grad_input, grad_up, grad_gain = pl.pallas_call(
        deliver,
        out_shape=tuple(jax.ShapeDtypeStruct(*shape) for shape in shapes),
        in_specs=[pl.BlockSpec(memory_space=pltpu.VMEM)] * 3,
        out_specs=(pl.BlockSpec(memory_space=pl.ANY),) * 3,
        scratch_shapes=[pltpu.SemaphoreType.DMA((3,))],
        name="deliver",
    )(*results)
    return grad_input, grad_up, grad_gain.reshape(half)


def deliver(*refs):
    *refs, sems = refs
    copies = [
        pltpu.make_async_copy(refs[i], refs[3 + i], sems.at[i]) for i in range(3)
    ]
    for copy in copies:
        copy.start()
    for copy in copies:
        copy.wait()


def in_kernel(*args):
    return kernel_step(lax.axis_size("fs"), lax.axis_size("tp"), *args)


def solution(mesh):
    placed = (
        P("fs", "tp"),
        P("fs", "tp"),
        P("fs", "tp"),
        P("tp"),
        P("tp", "fs"),
        P("tp", "fs"),
        P("fs", "tp"),
    )
    fs, tp = mesh.shape["fs"], mesh.shape["tp"]
    out_specs = (P("fs", "tp"), P("tp", "fs"), P("tp"))

    def solve(*args):
        up, down = args[4].shape, args[5].shape
        whole = up[1] // fs % 128 == 0 and down[1] // fs % 128 == 0
        if tp == 2 and fs == 4 * PLAN_STEPS and whole:
            return jax.shard_map(
                in_kernel, mesh=mesh, in_specs=placed, out_specs=out_specs, check_vma=False
            )(*args)
        return permuted(*args)

    step = jax.shard_map(
        on_device,
        mesh=mesh,
        in_specs=placed,
        out_specs=(P("fs", "tp"), P("tp", "fs"), P("tp")),
        check_vma=False,
    )
    permuted = step
    return solve
```
